32 devices in a mesh: ep: 8 (over z, core), tp: 4 (over y, x).
Axes of the slice: x: 2, y: 2, z: 4, core: 2. Of those that a mesh axis runs over, the one named last changes fastest.
Arguments:
- mixer_rows: bfloat16 [2048, 2048], P('ep'), may hold values from -8 to 8
- mixer_gain: float32 [2048], replicated, may hold values from 0.1 to 1.9
- w_query: bfloat16 [2048, 1024], P(None, 'tp'), may hold values from -0.125 to 0.125
- w_key: bfloat16 [2048, 1024], P(None, 'tp'), may hold values from -0.125 to 0.125
- w_value: bfloat16 [2048, 1024], P(None, 'tp'), may hold values from -0.125 to 0.125
- key_shift: float32 [16, 2048], P('tp'), may hold values from -14 to 0
- w_out: bfloat16 [1024, 2048], P(None, 'tp'), may hold values from -0.75 to 0.75
- expert_rows: bfloat16 [1024, 2048], P('ep'), may hold values from -6 to 6
- expert_gain: float32 [2048], replicated, may hold values from 0.1 to 1.9
- routes: int32 [1024, 4], P('ep'), may hold values from 0 to 7, all different within a row; in each aligned block of 128 rows (0 to 127, 128 to 255, ...) at most 128 rows name the same one
- route_weight: float32 [1024, 4], P('ep'), may hold values from 0.05 to 0.6
- w_gate: bfloat16 [8, 2048, 2048], P('ep', None, 'tp'), may hold values from -0.25 to 0.25
- w_up: bfloat16 [8, 2048, 2048], P('ep', None, 'tp'), may hold values from -0.25 to 0.25
- w_down: bfloat16 [8, 2048, 2048], P('ep', None, 'tp'), may hold values from -0.0625 to 0.0625
Outputs:
- mixer_out: bfloat16 [2048, 2048], P('ep', 'tp')
- expert_out: bfloat16 [1024, 2048], P('ep', 'tp')
The draws below stay inside these ranges and needn't reach their ends.
Inputs may be any that keep to these rules, and one draw needn't show every extreme that they name: `routes`: each row names 4 different experts. In each aligned block of 128 rows no expert is named by more than 128 rows, and in every draw some block names some expert exactly 128 times.
All inputs are finite; a program needn't handle non-finite values.
Results may differ from the reference program's by a relative error of at most 0.0073.
Values may be sent and summed in bfloat16 or wider, within the bound.
A program may use at most 64 MiB of HBM per device.

```python
import math
import jax
import jax.numpy as jnp
import numpy as np
from jax import lax

D = 2048
HEAD_TOTAL = 16
HEAD_DIM = 64
FF = 2048
TOPK = 4
TOKA_DEV = 256
TOKB_DEV = 128
SEQUENCE_TOKENS = 2048
TOKB = 1024
EXPERTS = 8
CAP = 128
N_EP = 8


def draw_mixer_rows(key, part):
    parallel_lanes = jax.random.split(key, 2)
    block_count = SEQUENCE_TOKENS // TOKA_DEV
    baseline = jax.random.normal(parallel_lanes[0], (SEQUENCE_TOKENS, D), jnp.float32)
    common = jax.random.normal(parallel_lanes[1], (block_count, D), jnp.float32)
    values = baseline + jnp.repeat(common, TOKA_DEV, axis=0)
    return jnp.clip(values, -8.0, 8.0).astype(jnp.bfloat16)


def draw_key_shift(key, part):
    parallel_lanes = jax.random.split(key, 7)
    block_count = SEQUENCE_TOKENS // TOKA_DEV
    fast_share = 0.5
    head_pick = jax.random.uniform(parallel_lanes[0], (HEAD_TOTAL, 1), jnp.float32)
    fast_span = jnp.exp(jax.random.uniform(parallel_lanes[1], (HEAD_TOTAL, 1), jnp.float32, 3.4, 4.6))
    slow_span = SEQUENCE_TOKENS * jax.random.uniform(parallel_lanes[2], (HEAD_TOTAL, 1), jnp.float32, 1.0, 2.0)
    baseline = -jnp.log(jnp.where(head_pick < fast_share, fast_span, slow_span))
    block_level = jax.random.uniform(parallel_lanes[3], (HEAD_TOTAL, block_count), jnp.float32, -0.7, 0.7)
    roughness = jax.random.uniform(parallel_lanes[4], (HEAD_TOTAL, SEQUENCE_TOKENS), jnp.float32, -0.5, 0.5)
    displaced_values = baseline + jnp.repeat(block_level, TOKA_DEV, axis=1) + roughness
    surge_selection = jax.random.uniform(parallel_lanes[5], (1, SEQUENCE_TOKENS), jnp.float32) < 4.0 / SEQUENCE_TOKENS
    surge_degree = jax.random.uniform(parallel_lanes[6], (HEAD_TOTAL, SEQUENCE_TOKENS), jnp.float32, -1.4, 0.0)
    return jnp.where(surge_selection, surge_degree, displaced_values).astype(jnp.float32)


def steps_of(own_key, extent, cuts, least, largest):
    loudness = 1.0
    for position, shards_of in cuts:
        draws = jax.random.uniform(jax.random.fold_in(jax.random.fold_in(own_key, 6), position), (shards_of,), jnp.float32, least / len(cuts), largest / len(cuts))
        loudness = loudness * jnp.repeat(jnp.exp(draws), extent[position] // shards_of).reshape((-1,) + (1,) * (len(extent) - 1 - position))
    return loudness


def shared_out(key, own, number, rows, number_of, top, reach, slope):
    sequence = jax.random.permutation(key, number_of)
    crowded, usual = shares(number_of, rows * top, reach, slope, True), shares(number_of, rows * top, reach, slope, False)
    places = jnp.arange(number_of)

    def named(lengths, turn):
        used = int((lengths > 0).sum())
        fixed = max(1, used // 4)
        passed = fixed + (places - fixed + turn * (used - fixed)) % max(1, number_of - fixed)
        return jnp.zeros((number_of,), jnp.int32).at[sequence[jnp.where(places < fixed, places, passed)]].set(jnp.asarray(lengths, jnp.int32))

    lengths = jnp.where(number % 4 == 0, named(crowded, number // 4), named(usual, number - number // 4 - 1))
    mixed = jax.random.permutation(jax.random.fold_in(own, 3), number_of)
    source_of, sink = mixed[0:number_of // 2 * 2:2], mixed[1:number_of // 2 * 2:2]
    slack = jnp.minimum(lengths[source_of] - 1, reach - lengths[sink]) // 2
    slack = jnp.where((source_of == sequence[0]) | (sink == sequence[0]) | (lengths[sink] == 0), 0, jnp.maximum(slack, 0))
    passed = jax.random.randint(jax.random.fold_in(own, 4), (number_of // 2,), 0, 1 << 20) % (slack + 1)
    lengths = lengths.at[source_of].add(-passed).at[sink].add(passed)
    labels = jnp.searchsorted(jnp.cumsum(lengths), jnp.arange(rows * top), side="right").astype(jnp.int32)
    grid = labels.reshape(top, rows).T
    grid = grid[jax.random.permutation(jax.random.fold_in(own, 1), rows)]
    turn = jax.random.randint(jax.random.fold_in(own, 2), (rows, 1), 0, top)
    return jnp.take_along_axis(grid, (jnp.arange(top)[None, :] + turn) % top, axis=1)


def shares(amount, total, reach, slope, full):
    portions = [(1 << 20) // math.isqrt(rank ** slope) + 1 for rank in range(1, amount + 1)]
    largest = reach if full else min(reach, max(-(-total // amount), total * portions[0] // sum(portions)))
    least = 1 if total - largest >= amount - 1 else 0
    holding, spare = [largest] + [least] * (amount - 1), total - largest - least * (amount - 1)
    while spare > 0:
        movable = [i for i in range(1, amount) if holding[i] < largest] or [i for i in range(1, amount) if holding[i] < reach]
        mass, left = sum([portions[i] for i in movable]), spare
        for i in movable:
            more = min(reach - holding[i], max(1, left * portions[i] // mass), spare)
            holding[i] = holding[i] + more
            spare = spare - more
    return np.array(holding)


def gaussian(key, extent, deviation, reach, cuts=(), held_as=jnp.bfloat16):
    array = deviation * jax.random.normal(key, extent, jnp.float32)
    if cuts:
        array = array * steps_of(key, extent, cuts, -0.22, 0.18)
    return jnp.clip(array, -reach, reach).astype(held_as)


def setup_inputs(seed: int = 0) -> dict:
    streams_of = jax.random.split(jax.random.key(seed), 15)
    mixer_rows = draw_mixer_rows(jax.random.fold_in(streams_of[14], 71), 0)
    mixer_gain = jnp.clip(1.0 + 0.18 * jax.random.normal(streams_of[1], (D,), jnp.float32), 0.1, 1.9)
    w_query = gaussian(streams_of[2], (D, HEAD_TOTAL * HEAD_DIM), D ** -0.5, 0.125, ((1, 4),))
    w_key = gaussian(streams_of[3], (D, HEAD_TOTAL * HEAD_DIM), D ** -0.5, 0.125, ((1, 4),))
    w_value = gaussian(streams_of[4], (D, HEAD_TOTAL * HEAD_DIM), D ** -0.5, 0.125, ((1, 4),))
    key_shift = draw_key_shift(jax.random.fold_in(streams_of[14], 71), 0)
    w_out = gaussian(streams_of[6], (HEAD_TOTAL * HEAD_DIM, D), (HEAD_TOTAL * HEAD_DIM // 16) ** -0.5, 0.75, ((1, 4),))
    expert_rows = gaussian(streams_of[7], (TOKB, D), 1.0, 6.0, ((0, 8),))
    expert_gain = jnp.clip(1.0 + 0.18 * jax.random.normal(streams_of[8], (D,), jnp.float32), 0.1, 1.9)
    routes_keys = jax.random.split(jax.random.fold_in(streams_of[9], 1), TOKB // TOKB_DEV)
    routes_turns = jax.random.permutation(jax.random.fold_in(streams_of[9], 3), TOKB // TOKB_DEV)
    routes = jax.vmap(lambda own, number: shared_out(jax.random.fold_in(streams_of[9], 2), own, number, TOKB_DEV, EXPERTS, TOPK, CAP, 2))(routes_keys, routes_turns).reshape((TOKB, TOPK))
    route_weight = jnp.clip(0.05 + 0.55 * jax.random.uniform(streams_of[10], (TOKB, TOPK), jnp.float32) ** steps_of(streams_of[10], (TOKB, TOPK), ((0, 8),), -0.2, 0.2), 0.05, 0.6)
    w_gate = gaussian(streams_of[11], (EXPERTS, D, FF), (D // 4) ** -0.5, 0.25, ((0, 8), (2, 4)))
    w_up = gaussian(streams_of[12], (EXPERTS, D, FF), (D // 4) ** -0.5, 0.25, ((0, 8), (2, 4)))
    w_down = gaussian(streams_of[13], (EXPERTS, FF, D), (4 * FF) ** -0.5, 0.0625, ((0, 8), (2, 4)))
    return {"mixer_rows": mixer_rows, "mixer_gain": mixer_gain, "w_query": w_query, "w_key": w_key, "w_value": w_value, "key_shift": key_shift, "w_out": w_out, "expert_rows": expert_rows, "expert_gain": expert_gain, "routes": routes, "route_weight": route_weight, "w_gate": w_gate, "w_up": w_up, "w_down": w_down}


norm_eps = 1e-06
glu_limit = 7.0
glu_alpha = 1.702

def rms_scale(source, scaling):
    floats = source.astype(jnp.float32)
    inverse = lax.rsqrt(lax.optimization_barrier(jnp.mean(floats * floats, axis=-1, keepdims=True)) + norm_eps)
    return (floats * inverse * scaling).astype(jnp.bfloat16)

def mixer_layer(mixer_rows, mixer_gain, w_query, w_key, w_value, key_shift, w_out):
    normed = rms_scale(mixer_rows, mixer_gain)
    total_rows = normed.shape[0]

    def project(weight):
        flat_out = jnp.dot(normed, weight, preferred_element_type=jnp.float32).astype(jnp.bfloat16)
        return flat_out.reshape(total_rows, HEAD_TOTAL, HEAD_DIM).transpose(1, 0, 2)
    positions = jnp.arange(total_rows, dtype=jnp.int32)
    block_starts = jnp.arange(total_rows // TOKA_DEV, dtype=jnp.int32) * TOKA_DEV

    def one_head(operands):
        query_head, key_head, value_head, shift_head = operands

        def one_block(begin_at):
            query_block = lax.dynamic_slice_in_dim(query_head, begin_at, TOKA_DEV, 0)
            query_pos = begin_at + jnp.arange(TOKA_DEV, dtype=jnp.int32)
            strict = positions[None, :] < query_pos[:, None]
            scores = jnp.dot(query_block, key_head.T, preferred_element_type=jnp.float32) * HEAD_DIM ** (-0.5)
            scores = scores + shift_head[None, :]
            log_stay = jnp.where(strict, jax.nn.log_sigmoid(-scores), 0.0)
            between = lax.cumsum(log_stay, axis=1, reverse=True) - log_stay
            weights = jnp.where(strict, jnp.exp(jax.nn.log_sigmoid(scores) + between), 0.0).astype(jnp.bfloat16)
            return jnp.dot(weights, value_head, preferred_element_type=jnp.float32).astype(jnp.bfloat16)
        return lax.map(one_block, block_starts).reshape(total_rows, HEAD_DIM)
    heads_out = lax.map(one_head, (project(w_query), project(w_key), project(w_value), key_shift))
    head_out = heads_out.transpose(1, 0, 2).reshape(total_rows, HEAD_TOTAL * HEAD_DIM)
    return jnp.dot(head_out, w_out, preferred_element_type=jnp.float32).astype(jnp.bfloat16)

def expert_layer(expert_rows, expert_gain, routes, route_weight, w_gate, w_up, w_down):
    normed = rms_scale(expert_rows, expert_gain)
    tokens_all = normed.shape[0]
    chosen = routes.reshape(-1).astype(jnp.int32)
    hit_table = (chosen[:, None] == jnp.arange(EXPERTS, dtype=jnp.int32)[None, :]).astype(jnp.int32)
    places = lax.optimization_barrier(jnp.sum((jnp.cumsum(hit_table, axis=0) - 1) * hit_table, axis=1)).astype(jnp.int32)
    room_size = N_EP * CAP
    targets = chosen * room_size + places
    assign_ids = jnp.arange(tokens_all * TOPK, dtype=jnp.int32) // TOPK
    owners = jnp.full((EXPERTS * room_size,), tokens_all, jnp.int32).at[targets].set(assign_ids)
    padded = jnp.concatenate([normed, jnp.zeros((1, D), jnp.bfloat16)], axis=0)

    def one_expert(operands):
        slot_ids, gate_cols, upper_cols, down_rows = operands
        picked_rows = padded[slot_ids]
        gating = jnp.minimum(jnp.dot(picked_rows, gate_cols, preferred_element_type=jnp.float32), glu_limit)
        linear = jnp.clip(jnp.dot(picked_rows, upper_cols, preferred_element_type=jnp.float32), -glu_limit, glu_limit)
        hidden = (gating * jax.nn.sigmoid(glu_alpha * gating) * (linear + 1.0)).astype(jnp.bfloat16)
        return jnp.dot(hidden, down_rows, preferred_element_type=jnp.float32).astype(jnp.bfloat16)
    results = lax.map(one_expert, (owners.reshape(EXPERTS, room_size), w_gate, w_up, w_down))
    picked = results.reshape(EXPERTS * room_size, D)[targets].astype(jnp.float32) * route_weight.reshape(-1)[:, None]
    return lax.optimization_barrier(jnp.sum(picked.reshape(tokens_all, TOPK, D), axis=1)).astype(jnp.bfloat16)

def reference(mixer_rows, mixer_gain, w_query, w_key, w_value, key_shift, w_out, expert_rows, expert_gain, routes, route_weight, w_gate, w_up, w_down):
    mixer_out = mixer_layer(mixer_rows, mixer_gain, w_query, w_key, w_value, key_shift, w_out)
    expert_out = expert_layer(expert_rows, expert_gain, routes, route_weight, w_gate, w_up, w_down)
    return (mixer_out, expert_out)
```

```python
import functools

import jax
import jax.numpy as jnp
from jax import lax
from jax.experimental import pallas as pl
from jax.experimental.pallas import tpu as pltpu
from jax.sharding import PartitionSpec as P

norm_eps = 1e-06
glu_limit = 7.0
glu_alpha = 1.702
HALF_FROM = 2
KV_SLOT = 0


def rms_scale(source, scaling):
    floats = source.astype(jnp.float32)
    inverse = lax.rsqrt(jnp.mean(floats * floats, axis=-1, keepdims=True) + norm_eps)
    return (floats * inverse * scaling).astype(jnp.bfloat16)


def stick_kernel(head_count, head_width, where_ref, q_ref, kv_ref, shift_ref, out_ref, acc, carry, upper):
    length = q_ref.shape[0]
    device = where_ref[0]
    group = min(head_count, max(1, 128 // head_width))
    span = group * head_width
    cols = head_count * head_width
    rows_i = lax.broadcasted_iota(jnp.int32, (length, length), 0)
    cols_i = lax.broadcasted_iota(jnp.int32, (length, length), 1)
    upper[...] = jnp.where(rows_i >= cols_i, 1.0, 0.0).astype(jnp.bfloat16)
    lane_owner = lax.broadcasted_iota(jnp.int32, (length, span), 1) // head_width

    def block(number, diagonal):
        base = pl.multiple_of(number * length, length)
        half = kv_ref.shape[0] // length // 2
        own_line = (device - number) % 2 == 0
        sibling = device + 1 - 2 * (device % 2)
        slot = jnp.where(own_line, (device - number) // 2, half + (sibling - number) // 2)
        start = pl.multiple_of(slot * length, length)
        for first in range(0, head_count, group):
            lanes = first * head_width
            pair_q = q_ref[:, lanes : lanes + span]
            pair_k = kv_ref[pl.ds(start, length), lanes : lanes + span]
            pair_v = kv_ref[pl.ds(start, length), cols + lanes : cols + lanes + span]
            merged = None
            for inside in range(group):
                head = first + inside
                mine = lane_owner == inside
                q_here = jnp.where(mine, pair_q, jnp.zeros_like(pair_q)) if group > 1 else pair_q
                scores = lax.dot_general(
                    q_here, pair_k, (((1,), (1,)), ((), ())), preferred_element_type=jnp.float32
                )
                scores = scores * head_width ** (-0.5) + shift_ref[head : head + 1, pl.ds(base, length)]
                stay = jnp.minimum(-scores, 0.0) - jnp.log(1.0 + jnp.exp(-jnp.abs(scores)))
                if diagonal:
                    stay = jnp.where(cols_i < rows_i, stay, 0.0)
                high = stay.astype(jnp.bfloat16)
                low = (stay - high.astype(jnp.float32)).astype(jnp.bfloat16)
                inclusive = jnp.dot(high, upper[...], preferred_element_type=jnp.float32)
                inclusive = inclusive + jnp.dot(low, upper[...], preferred_element_type=jnp.float32)
                if diagonal:
                    weights = jnp.where(cols_i < rows_i, jnp.exp(scores + inclusive), 0.0)
                    carry[:, head : head + 1] = inclusive[:, 0:1]
                else:
                    before = carry[:, head : head + 1]
                    weights = jnp.exp(scores + (inclusive + before))
                    carry[:, head : head + 1] = before + inclusive[:, 0:1]
                product = jnp.dot(
                    weights.astype(jnp.bfloat16), pair_v, preferred_element_type=jnp.float32
                )
                merged = product if merged is None else jnp.where(mine, product, merged)
            if diagonal:
                acc[:, lanes : lanes + span] = merged
            else:
                acc[:, lanes : lanes + span] += merged

    block(device, True)

    def earlier(step, nothing):
        block(device - 1 - step, False)
        return nothing

    lax.fori_loop(0, device, earlier, 0)
    out_ref[...] = acc[...].astype(out_ref.dtype)


def stick_block(head_count, head_width, number, slot, diagonal, q_ref, kv_ref, shift_ref, acc, carry, upper):
    length = q_ref.shape[0]
    group = min(head_count, max(1, 128 // head_width))
    span = group * head_width
    cols = head_count * head_width
    rows_i = lax.broadcasted_iota(jnp.int32, (length, length), 0)
    cols_i = lax.broadcasted_iota(jnp.int32, (length, length), 1)
    lane_owner = lax.broadcasted_iota(jnp.int32, (length, span), 1) // head_width
    base = pl.multiple_of(number * length, length)
    for first in range(0, head_count, group):
        lanes = first * head_width
        pair_q = q_ref[:, lanes : lanes + span]
        pair_k = kv_ref[slot, :, lanes : lanes + span]
        pair_v = kv_ref[slot, :, cols + lanes : cols + lanes + span]
        merged = None
        for inside in range(group):
            head = first + inside
            mine = lane_owner == inside
            q_here = jnp.where(mine, pair_q, jnp.zeros_like(pair_q)) if group > 1 else pair_q
            scores = lax.dot_general(
                q_here, pair_k, (((1,), (1,)), ((), ())), preferred_element_type=jnp.float32
            )
            scores = scores * head_width ** (-0.5) + shift_ref[head : head + 1, pl.ds(base, length)]
            stay = jnp.minimum(-scores, 0.0) - jnp.log(1.0 + jnp.exp(-jnp.abs(scores)))
            if diagonal:
                stay = jnp.where(cols_i < rows_i, stay, 0.0)
            high = stay.astype(jnp.bfloat16)
            low = (stay - high.astype(jnp.float32)).astype(jnp.bfloat16)
            inclusive = jnp.dot(high, upper[...], preferred_element_type=jnp.float32)
            inclusive = inclusive + jnp.dot(low, upper[...], preferred_element_type=jnp.float32)
            if diagonal:
                weights = jnp.where(cols_i < rows_i, jnp.exp(scores + inclusive), 0.0)
                carry[:, head : head + 1] = inclusive[:, 0:1]
            else:
                before = carry[:, head : head + 1]
                weights = jnp.exp(scores + (inclusive + before))
                carry[:, head : head + 1] = before + inclusive[:, 0:1]
            product = jnp.dot(
                weights.astype(jnp.bfloat16), pair_v, preferred_element_type=jnp.float32
            )
            merged = product if merged is None else jnp.where(mine, product, merged)
        if diagonal:
            acc[:, lanes : lanes + span] = merged
        else:
            acc[:, lanes : lanes + span] += merged


def fused_kernel(
    chips,
    head_count,
    head_width,
    mixer_hbm,
    mixer_gain,
    query_hbm,
    key_hbm,
    value_hbm,
    shift_hbm,
    out_hbm,
    expert_hbm,
    expert_gain,
    routes_ref,
    share_ref,
    gate_hbm,
    up_hbm,
    down_hbm,
    mixer_out,
    expert_out,
    mix_in,
    exp_in,
    normed,
    wq,
    wk,
    wv,
    shift,
    wo,
    wg,
    wu,
    wd,
    rows,
    hidden,
    part,
    part_in,
    pair_out,
    pair_keep,
    pair_in,
    done_out,
    done_keep,
    done_in,
    queries,
    kv,
    heads,
    acc,
    carry,
    upper,
    load_sem,
    far_sem,
    side_sem,
    mate_sem,
    unit_sem,
    part_sem,
    pair_sem,
    done_sem,
    kv_sem,
    head_sem,
    down_sem,
):
    ep, tp = lax.axis_index("ep"), lax.axis_index("tp")
    z, c = ep // 2, ep % 2
    y, x = tp // 2, tp % 2
    tokens, width = exp_in.shape
    length = mix_in.shape[0]
    units = wg.shape[1]
    half = tokens // 2
    cols = head_count * head_width
    mate = {"ep": 2 * z + 1 - c}
    beside = {"tp": 2 * y + 1 - x}
    across = {"tp": 2 * (1 - y) + x}

    def chip_core(chip):
        return {"ep": 2 * chip + c}

    def send(source, target, sems, number, device):
        return pltpu.make_async_remote_copy(
            src_ref=source,
            dst_ref=target,
            send_sem=sems.at[0, number],
            recv_sem=sems.at[1, number],
            device_id=device,
            device_id_type=pl.DeviceIdType.MESH,
        )

    def load(number, source, target):
        return pltpu.make_async_copy(source, target, load_sem.at[number])

    loads = [
        load(0, expert_hbm, exp_in),
        load(1, mixer_hbm, mix_in),
        load(2, query_hbm, wq),
        load(3, key_hbm, wk),
        load(4, value_hbm, wv),
        load(5, shift_hbm, shift),
        load(6, gate_hbm.at[0], wg),
        load(7, up_hbm.at[0], wu),
        load(8, down_hbm.at[0, pl.ds(units * x, units), :], wd.at[x, 0]),
        load(9, down_hbm.at[0, pl.ds(units * (2 + x), units), :], wd.at[x, 1]),
        load(10, out_hbm, wo),
    ]
    for copy in loads[:8]:
        copy.start()

    barrier = pltpu.get_barrier_semaphore()
    pl.semaphore_signal(barrier, inc=1, device_id=mate, device_id_type=pl.DeviceIdType.MESH)
    for step in range(1, 4):
        pl.semaphore_signal(
            barrier, inc=1, device_id={"tp": (tp + step) % 4}, device_id_type=pl.DeviceIdType.MESH
        )
    for step in range(1, chips):
        pl.semaphore_signal(
            barrier,
            inc=1,
            device_id=chip_core((z + step) % chips),
            device_id_type=pl.DeviceIdType.MESH,
        )

    mine = pl.ds(pl.multiple_of(c * tokens, tokens), tokens)
    lanes_i = lax.broadcasted_iota(jnp.int32, (128, 128), 0)
    table = jnp.zeros((128, tokens), jnp.float32)
    for slot in range(routes_ref.shape[0]):
        table = table + jnp.where(
            lanes_i % (2 * chips) == routes_ref[slot : slot + 1, :], share_ref[slot : slot + 1, :], 0.0
        )
    high = table.astype(jnp.bfloat16).astype(jnp.float32)
    table = jnp.where(lanes_i < 2 * chips, high, jnp.where(lanes_i < 4 * chips, table - high, 0.0))
    loads[0].wait()
    step_rows = 32

    def norm_tokens(index, nothing):
        at = pl.multiple_of(index * step_rows, step_rows)
        rows[z, pl.ds(pl.multiple_of(c * tokens + at, step_rows), step_rows), :width] = rms_scale(
            exp_in[pl.ds(at, step_rows), :], expert_gain[...]
        )
        return nothing

    lax.fori_loop(0, tokens // step_rows, norm_tokens, 0, unroll=2)
    rows[z, mine, width:] = table.T.astype(jnp.bfloat16)

    pl.semaphore_wait(barrier, 3 + chips)

    def own_rows(chip):
        return rows.at[chip, mine, :]

    def half_rows(chip, which):
        return rows.at[chip, pl.ds(pl.multiple_of(c * tokens + which * half, half), half), :]

    def mate_rows(chip):
        return send(own_rows(chip), own_rows(chip), mate_sem, chip, mate)

    def far_copy(part_rows, chip, target):
        return pltpu.make_async_remote_copy(
            src_ref=part_rows,
            dst_ref=part_rows,
            send_sem=far_sem.at[jnp.where(target > z, 1, 0), chip],
            recv_sem=far_sem.at[2, chip],
            device_id=chip_core(target % chips),
            device_id_type=pl.DeviceIdType.MESH,
        )

    def far_full(chip, target):
        return far_copy(own_rows(chip), chip, target)

    def far_half(chip, target):
        return far_copy(half_rows(chip, y), chip, target)

    def side_half(chip):
        return send(half_rows(chip, y), half_rows(chip, y), side_sem, chip, across)

    def is_full(chip, target):
        return jnp.abs(chip - target) < HALF_FROM

    def far(chip, target, act):
        if HALF_FROM <= 1:
            act(far_half(chip, target))
        else:
            pl.when(is_full(chip, target))(lambda: act(far_full(chip, target)))
            pl.when(jnp.logical_not(is_full(chip, target)))(lambda: act(far_half(chip, target)))

    def start(copy):
        copy.start()

    up_ok, down_ok = z < chips - 1, z > 0
    pl.when(up_ok)(lambda: far(z, z + 1, start))
    pl.when(down_ok)(lambda: far(z, z - 1, start))
    mate_rows(z).start()

    def down_piece(number):
        return send(
            down_hbm.at[0, pl.ds(units * (2 * number + 1 - x), units), :],
            wd.at[x, number],
            down_sem,
            number,
            beside,
        )

    down_piece(0).start()
    down_piece(1).start()
    for copy in loads[8:]:
        copy.start()

    loads[1].wait()

    def norm_mixer(index, nothing):
        at = pl.ds(pl.multiple_of(index * step_rows, step_rows), step_rows)
        normed[at, :] = rms_scale(mix_in[at, :], mixer_gain[...])
        return nothing

    lax.fori_loop(0, length // step_rows, norm_mixer, 0, unroll=2)

    def kv_far(chip):
        return send(kv.at[2 * chip + c], kv.at[2 * chip + c], kv_sem.at[0], chip, chip_core((z + 1) % chips))

    def kv_mate(chip):
        return send(kv.at[2 * chip + c], kv.at[2 * chip + c], kv_sem.at[1], chip, mate)

    loads[3].wait()
    kv[ep, :, :cols] = jnp.dot(normed[...], wk[...], preferred_element_type=jnp.float32).astype(jnp.bfloat16)
    loads[4].wait()
    kv[ep, :, cols:] = jnp.dot(normed[...], wv[...], preferred_element_type=jnp.float32).astype(jnp.bfloat16)
    if KV_SLOT == 0:
        pl.when(up_ok)(lambda: kv_far(z).start())
    kv_mate(z).start()
    loads[2].wait()
    queries[...] = jnp.dot(normed[...], wq[...], preferred_element_type=jnp.float32).astype(jnp.bfloat16)
    rows_i = lax.broadcasted_iota(jnp.int32, (length, length), 0)
    cols_i = lax.broadcasted_iota(jnp.int32, (length, length), 1)
    upper[...] = jnp.where(rows_i >= cols_i, 1.0, 0.0).astype(jnp.bfloat16)
    loads[5].wait()

    def attend(number, diagonal):
        stick_block(
            head_count, head_width, number, number, diagonal, queries, kv, shift, acc, carry, upper
        )

    near = jnp.minimum(z, chips - 1 - z)

    def chip_at(step):
        index = step - 1
        both = index < 2 * near
        distance = jnp.where(both, index // 2 + 1, index - near + 1)
        below = jnp.where(both, index % 2 == 0, z > chips - 1 - z)
        return jnp.where(step == 0, z, jnp.where(below, z - distance, z + distance))

    def stage_rows(step):
        chip = chip_at(step)
        from_below = chip < z
        target = jnp.where(from_below, z + 1, z - 1)
        far(chip, z, lambda copy: copy.wait_recv())
        pl.when((target >= 0) & (target < chips))(lambda: far(chip, target, start))
        full = is_full(chip, z)
        if HALF_FROM > 1:
            pl.when(full)(lambda: mate_rows(chip).start())
        pl.when(jnp.logical_not(full))(lambda: side_half(chip).start())

    def stage_side(step):
        chip = chip_at(step)

        @pl.when(jnp.logical_not(is_full(chip, z)))
        def _():
            side_half(chip).wait_recv()
            mate_rows(chip).start()

    def unit_copy(chip):
        return send(hidden.at[chip, y], hidden.at[chip, y], unit_sem, chip, across)

    def stage_units(step):
        chip = chip_at(step)
        mate_rows(chip).wait_recv()
        lane = lax.broadcasted_iota(jnp.int32, (2 * tokens, 128), 1)
        weight = jnp.sum(
            jnp.where(
                (lane == ep) | (lane == ep + 2 * chips), rows[chip, :, width:].astype(jnp.float32), 0.0
            ),
            axis=1,
            keepdims=True,
        )
        wide = 256
        for first in range(0, units, wide):
            at = slice(first, first + wide)
            gating = jnp.dot(rows[chip, :, :width], wg[:, at], preferred_element_type=jnp.float32)
            linear = jnp.dot(rows[chip, :, :width], wu[:, at], preferred_element_type=jnp.float32)
            gating = jnp.minimum(gating, glu_limit)
            linear = jnp.clip(linear, -glu_limit, glu_limit)
            value = gating * jax.nn.sigmoid(glu_alpha * gating) * (linear + 1.0)
            hidden[chip, y, :, at] = (value * weight).astype(jnp.bfloat16)
        unit_copy(chip).start()

    other_rows = pl.ds(pl.multiple_of((1 - c) * tokens, tokens), tokens)

    def part_copy(chip):
        return send(part.at[chip, :, other_rows, :], part_in.at[chip], part_sem, chip, mate)

    def stage_down(step):
        chip = chip_at(step)
        unit_copy(chip).wait_recv()
        for side in range(2):
            for first in range(0, wd.shape[3], 256):
                at = slice(first, first + 256)
                total = jnp.dot(
                    hidden[chip, 0], wd[side, 0, :, at], preferred_element_type=jnp.float32
                ) + jnp.dot(hidden[chip, 1], wd[side, 1, :, at], preferred_element_type=jnp.float32)
                part[chip, side, :, at] = total.astype(jnp.bfloat16)
        part_copy(chip).start()

    def pair_copy(chip):
        return send(pair_out.at[chip], pair_in.at[chip], pair_sem, chip, beside)

    def stage_pair(step):
        chip = chip_at(step)
        part_copy(chip).wait_recv()
        pair_out[chip] = (
            part[chip, 1 - x, mine, :].astype(jnp.float32) + part_in[chip, 1 - x].astype(jnp.float32)
        ).astype(jnp.bfloat16)
        pair_copy(chip).start()
        pair_keep[chip] = part[chip, x, mine, :].astype(jnp.float32) + part_in[chip, x].astype(jnp.float32)

    def done_copy(chip):
        return pltpu.make_async_remote_copy(
            src_ref=done_out.at[chip],
            dst_ref=done_in.at[z],
            send_sem=done_sem.at[0, chip],
            recv_sem=done_sem.at[1, z],
            device_id=chip_core(chip),
            device_id_type=pl.DeviceIdType.MESH,
        )

    def done_arrived(chip):
        return send(done_out.at[chip], done_in.at[chip], done_sem, chip, chip_core(chip))

    def stage_done(step):
        chip = chip_at(step)
        pair_copy(chip).wait_recv()
        total = pair_keep[chip] + pair_in[chip].astype(jnp.float32)

        @pl.when(chip == z)
        def _():
            done_keep[...] = total

        @pl.when(chip != z)
        def _():
            done_out[chip] = total.astype(jnp.bfloat16)
            done_copy(chip).start()

    def kv_arrive(back):
        chip = z - back
        kv_sent(chip).wait_recv()
        pl.when(up_ok)(lambda: kv_far(chip).start())
        kv_mate(chip).start()

    def kv_sent(chip):
        return send(kv.at[2 * chip + c], kv.at[2 * chip + c], kv_sem.at[0], chip, chip_core((z + 1) % chips))

    def kv_mate_arrived(chip):
        return send(kv.at[2 * chip + 1 - c], kv.at[2 * chip + 1 - c], kv_sem.at[1], chip, mate)

    def attend_chip(back):
        chip = z - back
        kv_mate_arrived(chip).wait_recv()

        @pl.when((back > 0) | (c == 1))
        def _():
            first = jnp.where(back > 0, 1, 0)

            def one(number, nothing):
                attend(2 * chip + first - number, False)
                return nothing

            lax.fori_loop(0, 1 + first, one, 0)

    attend(ep, True)

    def slot(step, nothing):
        more = step + 1 < chips
        pl.when(step < chips)(lambda: stage_units(step))
        pl.when(more)(lambda: stage_rows(step + 1))
        if KV_SLOT > 0:
            pl.when((step == KV_SLOT - 1) & up_ok)(lambda: kv_far(z).start())
        pl.when(step >= 1)(lambda: stage_down(step - 1))
        pl.when(more)(lambda: stage_side(step + 1))
        pl.when(step >= 2)(lambda: stage_done(step - 2))
        pl.when((step >= 1) & (step <= z))(lambda: kv_arrive(step))
        pl.when(step >= 1)(lambda: stage_pair(step - 1))
        pl.when((step >= 1) & (step - 1 <= z))(lambda: attend_chip(step - 1))
        return nothing

    loads[6].wait()
    loads[7].wait()

    def early(step, nothing):
        @pl.when(step == 1)
        def _():
            loads[8].wait()
            loads[9].wait()
            down_arrived(0).wait_recv()
            down_arrived(1).wait_recv()

        return slot(step, nothing)

    def down_arrived(number):
        return send(wd.at[1 - x, number], wd.at[1 - x, number], down_sem, number, beside)

    lax.fori_loop(0, chips + 1, early, 0)

    heads[tp] = acc[...].astype(jnp.bfloat16)

    def head_copy(step):
        other = (tp + step) % 4
        return pltpu.make_async_remote_copy(
            src_ref=heads.at[tp],
            dst_ref=heads.at[tp],
            send_sem=head_sem.at[0, other],
            recv_sem=head_sem.at[1, tp],
            device_id={"tp": other},
            device_id_type=pl.DeviceIdType.MESH,
        )

    for step in range(1, 4):
        head_copy(step).start()
    stage_done(chips - 1)
    loads[10].wait()
    for step in range(1, 4):
        other = (tp + step) % 4
        send(heads.at[other], heads.at[other], head_sem, other, {"tp": other}).wait_recv()
    for first in range(0, wo.shape[1], 256):
        at = slice(first, first + 256)
        total = jnp.zeros((length, 256), jnp.float32)
        for number in range(4):
            total = total + jnp.dot(
                heads[number], wo[number * cols : (number + 1) * cols, at], preferred_element_type=jnp.float32
            )
        mixer_out[:, at] = total.astype(mixer_out.dtype)
    total = done_keep[...]
    for step in range(1, chips):
        chip = (z + step) % chips
        done_arrived(chip).wait_recv()
        total = total + done_in[chip].astype(jnp.float32)
    expert_out[...] = total.astype(expert_out.dtype)

    def sent(copy):
        copy.wait_send()

    down_piece(0).wait_send()
    down_piece(1).wait_send()
    for step in range(1, 4):
        head_copy(step).wait_send()

    def drain(chip, nothing):
        pl.when((chip <= z) & up_ok)(lambda: far(chip, z + 1, sent))
        pl.when((chip >= z) & down_ok)(lambda: far(chip, z - 1, sent))
        pl.when(jnp.logical_not(is_full(chip, z)))(lambda: side_half(chip).wait_send())
        mate_rows(chip).wait_send()
        unit_copy(chip).wait_send()
        part_copy(chip).wait_send()
        pair_copy(chip).wait_send()
        pl.when(chip != z)(lambda: done_copy(chip).wait_send())
        pl.when((chip <= z) & up_ok)(lambda: kv_far(chip).wait_send())
        pl.when(chip <= z)(lambda: kv_mate(chip).wait_send())
        return nothing

    lax.fori_loop(0, chips, drain, 0)


def fused_layers(
    mixer_rows,
    mixer_gain,
    w_query,
    w_key,
    w_value,
    key_shift,
    w_out,
    expert_rows,
    expert_gain,
    routes,
    route_weight,
    w_gate,
    w_up,
    w_down,
):
    chips = lax.axis_size("ep") // 2
    length, width = mixer_rows.shape
    tokens = expert_rows.shape[0]
    head_count = key_shift.shape[0]
    cols = w_query.shape[1]
    units = w_gate.shape[2]
    outs = w_down.shape[2]
    b16, f32 = jnp.bfloat16, jnp.float32
    vmem = pl.BlockSpec(memory_space=pltpu.VMEM)
    hbm = pl.BlockSpec(memory_space=pl.ANY)
    dma = pltpu.SemaphoreType.DMA
    wide = width + 128
    return pl.pallas_call(
        functools.partial(fused_kernel, chips, head_count, cols // head_count),
        out_shape=(
            jax.ShapeDtypeStruct((length, w_out.shape[1]), b16),
            jax.ShapeDtypeStruct((tokens, outs), b16),
        ),
        in_specs=[hbm, vmem, hbm, hbm, hbm, hbm, hbm, hbm, vmem, vmem, vmem, hbm, hbm, hbm],
        out_specs=(vmem, vmem),
        scratch_shapes=[
            pltpu.VMEM((length, width), b16),
            pltpu.VMEM((tokens, width), b16),
            pltpu.VMEM((length, width), b16),
            pltpu.VMEM(w_query.shape, b16),
            pltpu.VMEM(w_key.shape, b16),
            pltpu.VMEM(w_value.shape, b16),
            pltpu.VMEM(key_shift.shape, f32),
            pltpu.VMEM(w_out.shape, b16),
            pltpu.VMEM(w_gate.shape[1:], b16),
            pltpu.VMEM(w_up.shape[1:], b16),
            pltpu.VMEM((2, 2, units, outs), b16),
            pltpu.VMEM((chips, 2 * tokens, wide), b16),
            pltpu.VMEM((chips, 2, 2 * tokens, units), b16),
            pltpu.VMEM((chips, 2, 2 * tokens, outs), b16),
            pltpu.VMEM((chips, 2, tokens, outs), b16),
            pltpu.VMEM((chips, tokens, outs), b16),
            pltpu.VMEM((chips, tokens, outs), f32),
            pltpu.VMEM((chips, tokens, outs), b16),
            pltpu.VMEM((chips, tokens, outs), b16),
            pltpu.VMEM((tokens, outs), f32),
            pltpu.VMEM((chips, tokens, outs), b16),
            pltpu.VMEM((length, cols), b16),
            pltpu.VMEM((2 * chips, length, 2 * cols), b16),
            pltpu.VMEM((4, length, cols), b16),
            pltpu.VMEM((length, cols), f32),
            pltpu.VMEM((length, max(128, head_count)), f32),
            pltpu.VMEM((length, length), b16),
            dma((11,)),
            dma((3, chips)),
            dma((2, chips)),
            dma((2, chips)),
            dma((2, chips)),
            dma((2, chips)),
            dma((2, chips)),
            dma((2, chips)),
            dma((2, 2, chips)),
            dma((2, 4)),
            dma((2, 2)),
        ],
        compiler_params=pltpu.CompilerParams(
            collective_id=0, has_side_effects=True, vmem_limit_bytes=60 * 1024 * 1024
        ),
    )(
        mixer_rows,
        mixer_gain.reshape(1, -1),
        w_query,
        w_key,
        w_value,
        key_shift,
        w_out,
        expert_rows,
        expert_gain.reshape(1, -1),
        routes.T,
        route_weight.T,
        w_gate,
        w_up,
        w_down,
    )


def earlier_blocks(packed, axis):
    size = lax.axis_size(axis)
    line = [packed]
    for shift in range(2, size, 2):
        line.append(lax.ppermute(packed, axis, [(i, i + shift) for i in range(size - shift)]))
    line = jnp.concatenate(line, axis=0)
    across = lax.ppermute(line, axis, [(i, i ^ 1) for i in range(size)])
    return jnp.concatenate([line, across], axis=0)


def stick_attention(device, queries, gathered, key_shift, head_width):
    length, cols = queries.shape
    head_count = key_shift.shape[0]
    total = gathered.shape[0]
    vmem = pl.BlockSpec(memory_space=pltpu.VMEM)
    return pl.pallas_call(
        functools.partial(stick_kernel, head_count, head_width),
        out_shape=jax.ShapeDtypeStruct((length, cols), jnp.bfloat16),
        in_specs=[pl.BlockSpec(memory_space=pltpu.SMEM), vmem, vmem, vmem],
        out_specs=vmem,
        scratch_shapes=[
            pltpu.VMEM((length, cols), jnp.float32),
            pltpu.VMEM((length, max(128, head_count)), jnp.float32),
            pltpu.VMEM((length, length), jnp.bfloat16),
        ],
        cost_estimate=pl.CostEstimate(
            flops=total * length * head_count * 1500,
            bytes_accessed=gathered.size * 2,
            transcendentals=total * length * head_count * 3,
        ),
    )(device.reshape(1).astype(jnp.int32), queries, gathered, key_shift)


def expert_hidden(flat_rows, gate_cols, upper_cols):
    gating = jnp.minimum(
        jnp.dot(flat_rows, gate_cols, preferred_element_type=jnp.float32), glu_limit
    )
    linear = jnp.clip(
        jnp.dot(flat_rows, upper_cols, preferred_element_type=jnp.float32), -glu_limit, glu_limit
    )
    return (gating * jax.nn.sigmoid(glu_alpha * gating) * (linear + 1.0)).astype(jnp.bfloat16)


def per_device(
    mixer_rows,
    mixer_gain,
    w_query,
    w_key,
    w_value,
    key_shift,
    w_out,
    expert_rows,
    expert_gain,
    routes,
    route_weight,
    w_gate,
    w_up,
    w_down,
):
    length = mixer_rows.shape[0]
    head_count = key_shift.shape[0]
    head_width = w_query.shape[1] // head_count
    if lax.axis_size("tp") == 4 and lax.axis_size("ep") <= 8 and expert_rows.shape[0] == 128:
        return fused_layers(
            mixer_rows,
            mixer_gain,
            w_query,
            w_key,
            w_value,
            key_shift,
            w_out,
            expert_rows,
            expert_gain,
            routes,
            route_weight,
            w_gate,
            w_up,
            w_down,
        )
    normed = rms_scale(mixer_rows, mixer_gain)
    queries = jnp.dot(normed, w_query, preferred_element_type=jnp.float32).astype(jnp.bfloat16)
    key_rows = jnp.dot(normed, w_key, preferred_element_type=jnp.float32).astype(jnp.bfloat16)
    value_rows = jnp.dot(normed, w_value, preferred_element_type=jnp.float32).astype(jnp.bfloat16)
    packed = jnp.concatenate([key_rows, value_rows], axis=1)
    device = lax.axis_index("ep")
    tokens_here, top_count = routes.shape
    expert_count = lax.axis_size("ep")
    capacity = 2 * tokens_here * top_count // expert_count
    rows_after_norm = rms_scale(expert_rows, expert_gain)
    dense = capacity >= tokens_here
    if dense:
        flat_rows = lax.all_gather(rows_after_norm, "ep", axis=0, tiled=True)
        flat_rows, packed, queries = lax.optimization_barrier((flat_rows, packed, queries))
    gathered = earlier_blocks(packed, "ep")
    head_out = stick_attention(device, queries, gathered, key_shift, head_width)
    if dense:
        hidden = expert_hidden(flat_rows, w_gate[0], w_up[0])
        units = lax.all_gather(hidden, "tp", axis=1, tiled=True)
        units, head_out = lax.optimization_barrier((units, head_out))
    weight_rows = w_out
    mixer_out = jnp.dot(
        lax.all_gather(head_out, "tp", axis=1, tiled=True),
        weight_rows,
        preferred_element_type=jnp.float32,
    ).astype(jnp.bfloat16)
    if dense:
        results = jnp.dot(units, w_down[0], preferred_element_type=jnp.float32).astype(jnp.bfloat16)
        leaving = results.reshape(expert_count, tokens_here, results.shape[1])
        returned = lax.all_to_all(leaving, "ep", split_axis=0, concat_axis=0, tiled=True)
        share = jnp.sum(
            jnp.where(
                routes[:, :, None] == jnp.arange(expert_count, dtype=jnp.int32)[None, None, :],
                route_weight[:, :, None],
                0.0,
            ),
            axis=1,
        )
        expert_out = jnp.zeros((tokens_here, results.shape[1]), jnp.float32)
        for number in range(expert_count):
            expert_out = expert_out + share[:, number : number + 1] * returned[number].astype(jnp.float32)
        return (mixer_out, expert_out.astype(jnp.bfloat16))
    chosen = routes.reshape(-1)
    hit_table = (chosen[:, None] == jnp.arange(expert_count, dtype=jnp.int32)[None, :]).astype(
        jnp.int32
    )
    places = jnp.sum((jnp.cumsum(hit_table, axis=0) - 1) * hit_table, axis=1)
    targets = chosen * capacity + places
    assign_ids = jnp.arange(tokens_here * top_count, dtype=jnp.int32) // top_count
    owners = (
        jnp.full((expert_count * capacity,), tokens_here, jnp.int32).at[targets].set(assign_ids)
    )
    padded = jnp.concatenate(
        [rows_after_norm, jnp.zeros((1, rows_after_norm.shape[1]), jnp.bfloat16)], axis=0
    )
    outgoing = padded[owners].reshape(expert_count, capacity, rows_after_norm.shape[1])
    gate_cols = w_gate[0]
    upper_cols = w_up[0]
    down_rows = w_down[0]
    arrived = lax.all_to_all(outgoing, "ep", split_axis=0, concat_axis=0, tiled=True)
    expert_senders, slots_here, feature_count = arrived.shape
    flat_rows = arrived.reshape(expert_senders * slots_here, feature_count)
    gating = jnp.minimum(
        jnp.dot(flat_rows, gate_cols, preferred_element_type=jnp.float32), glu_limit
    )
    linear = jnp.clip(
        jnp.dot(flat_rows, upper_cols, preferred_element_type=jnp.float32), -glu_limit, glu_limit
    )
    hidden = gating * jax.nn.sigmoid(glu_alpha * gating) * (linear + 1.0)
    hidden = hidden.astype(jnp.bfloat16).reshape(expert_senders, slots_here, gate_cols.shape[1])
    senders = hidden.shape[0]
    slot_total = hidden.shape[1]
    portion_units = lax.all_gather(hidden, "tp", axis=2, tiled=True)
    weight_rows = down_rows
    flat_units = portion_units.reshape(senders * slot_total, portion_units.shape[2])
    results = jnp.dot(flat_units, weight_rows, preferred_element_type=jnp.float32)
    leaving = results.astype(jnp.bfloat16).reshape(senders, slot_total, down_rows.shape[1])
    returned = lax.all_to_all(leaving, "ep", split_axis=0, concat_axis=0, tiled=True)
    picked = returned.reshape(expert_count * capacity, down_rows.shape[1])[targets].astype(
        jnp.float32
    )
    picked = picked * route_weight.reshape(-1)[:, None]
    expert_out = jnp.sum(picked.reshape(tokens_here, top_count, down_rows.shape[1]), axis=1).astype(
        jnp.bfloat16
    )
    return (mixer_out, expert_out)


def solution(mesh):
    placed = (
        P("ep", None),
        P(),
        P(None, "tp"),
        P(None, "tp"),
        P(None, "tp"),
        P("tp", None),
        P(None, "tp"),
        P("ep", None),
        P(),
        P("ep", None),
        P("ep", None),
        P("ep", None, "tp"),
        P("ep", None, "tp"),
        P("ep", None, "tp"),
    )
    return jax.shard_map(
        per_device,
        mesh=mesh,
        in_specs=placed,
        out_specs=(P("ep", "tp"), P("ep", "tp")),
        check_vma=False,
    )
```

```python
import functools

import jax
import jax.numpy as jnp
from jax import lax
from jax.experimental import pallas as pl
from jax.experimental.pallas import tpu as pltpu
from jax.sharding import PartitionSpec as P

norm_eps = 1e-06
glu_limit = 7.0
glu_alpha = 1.702
HALF_FROM = 1
WEIGHTS_AT = 33.0
SEND_DOWN_AT = 18.4
HEADS_AT = 44.0
KV_FROM = 3.3
KV_HOP = 7.0
KV_STEP = 5.7
ROWS_AT = (0.0, 9.5, 18.3, 25.8)
SIDE_AT = (0.0, 19.0, 24.5, 30.5)
KV_OWN_AT = (0.0, 9.6, 18.35, 0.0)
ATTEND_AT = (11.0, 32.5, 38.2, 43.8)
UNITS_AT = (7.7, 20.0, 26.0, 32.0)
DOWN_AT = (34.0, 34.7, 35.4, 41.0)
PAIR_AT = (36.2, 36.9, 37.6, 42.5)
DONE_AT = (40.5, 41.2, 44.1, 47.0)


def rms_scale(source, scaling):
    floats = source.astype(jnp.float32)
    inverse = lax.rsqrt(jnp.mean(floats * floats, axis=-1, keepdims=True) + norm_eps)
    return (floats * inverse * scaling).astype(jnp.bfloat16)


def stick_kernel(head_count, head_width, where_ref, q_ref, kv_ref, shift_ref, out_ref, acc, carry, upper):
    length = q_ref.shape[0]
    device = where_ref[0]
    group = min(head_count, max(1, 128 // head_width))
    span = group * head_width
    cols = head_count * head_width
    rows_i = lax.broadcasted_iota(jnp.int32, (length, length), 0)
    cols_i = lax.broadcasted_iota(jnp.int32, (length, length), 1)
    upper[...] = jnp.where(rows_i >= cols_i, 1.0, 0.0).astype(jnp.bfloat16)
    lane_owner = lax.broadcasted_iota(jnp.int32, (length, span), 1) // head_width

    def block(number, diagonal):
        base = pl.multiple_of(number * length, length)
        half = kv_ref.shape[0] // length // 2
        own_line = (device - number) % 2 == 0
        sibling = device + 1 - 2 * (device % 2)
        slot = jnp.where(own_line, (device - number) // 2, half + (sibling - number) // 2)
        start = pl.multiple_of(slot * length, length)
        for first in range(0, head_count, group):
            lanes = first * head_width
            pair_q = q_ref[:, lanes : lanes + span]
            pair_k = kv_ref[pl.ds(start, length), lanes : lanes + span]
            pair_v = kv_ref[pl.ds(start, length), cols + lanes : cols + lanes + span]
            merged = None
            for inside in range(group):
                head = first + inside
                mine = lane_owner == inside
                q_here = jnp.where(mine, pair_q, jnp.zeros_like(pair_q)) if group > 1 else pair_q
                scores = lax.dot_general(
                    q_here, pair_k, (((1,), (1,)), ((), ())), preferred_element_type=jnp.float32
                )
                scores = scores * head_width ** (-0.5) + shift_ref[head : head + 1, pl.ds(base, length)]
                stay = jnp.minimum(-scores, 0.0) - jnp.log(1.0 + jnp.exp(-jnp.abs(scores)))
                if diagonal:
                    stay = jnp.where(cols_i < rows_i, stay, 0.0)
                high = stay.astype(jnp.bfloat16)
                low = (stay - high.astype(jnp.float32)).astype(jnp.bfloat16)
                inclusive = jnp.dot(high, upper[...], preferred_element_type=jnp.float32)
                inclusive = inclusive + jnp.dot(low, upper[...], preferred_element_type=jnp.float32)
                if diagonal:
                    weights = jnp.where(cols_i < rows_i, jnp.exp(scores + inclusive), 0.0)
                    carry[:, head : head + 1] = inclusive[:, 0:1]
                else:
                    before = carry[:, head : head + 1]
                    weights = jnp.exp(scores + (inclusive + before))
                    carry[:, head : head + 1] = before + inclusive[:, 0:1]
                product = jnp.dot(
                    weights.astype(jnp.bfloat16), pair_v, preferred_element_type=jnp.float32
                )
                merged = product if merged is None else jnp.where(mine, product, merged)
            if diagonal:
                acc[:, lanes : lanes + span] = merged
            else:
                acc[:, lanes : lanes + span] += merged

    block(device, True)

    def earlier(step, nothing):
        block(device - 1 - step, False)
        return nothing

    lax.fori_loop(0, device, earlier, 0)
    out_ref[...] = acc[...].astype(out_ref.dtype)


def stick_block(head_count, head_width, number, slot, diagonal, q_ref, kv_ref, shift_ref, acc, carry, upper):
    length = q_ref.shape[0]
    group = min(head_count, max(1, 128 // head_width))
    span = group * head_width
    cols = head_count * head_width
    rows_i = lax.broadcasted_iota(jnp.int32, (length, length), 0)
    cols_i = lax.broadcasted_iota(jnp.int32, (length, length), 1)
    lane_owner = lax.broadcasted_iota(jnp.int32, (length, span), 1) // head_width
    base = pl.multiple_of(number * length, length)
    for first in range(0, head_count, group):
        lanes = first * head_width
        pair_q = q_ref[:, lanes : lanes + span]
        pair_k = kv_ref[slot, :, lanes : lanes + span]
        pair_v = kv_ref[slot, :, cols + lanes : cols + lanes + span]
        scores, sums = [], []
        for inside in range(group):
            head = first + inside
            q_here = jnp.where(lane_owner == inside, pair_q, jnp.zeros_like(pair_q)) if group > 1 else pair_q
            raw = lax.dot_general(q_here, pair_k, (((1,), (1,)), ((), ())), preferred_element_type=jnp.float32)
            scores.append(raw * head_width ** (-0.5) + shift_ref[head : head + 1, pl.ds(base, length)])
        for inside in range(group):
            score = scores[inside]
            stay = jnp.minimum(-score, 0.0) - jnp.log(1.0 + jnp.exp(-jnp.abs(score)))
            if diagonal:
                stay = jnp.where(cols_i < rows_i, stay, 0.0)
            high = stay.astype(jnp.bfloat16)
            low = (stay - high.astype(jnp.float32)).astype(jnp.bfloat16)
            sums.append(
                jnp.dot(jnp.concatenate([high, low], axis=1), upper[...], preferred_element_type=jnp.float32)
            )
        merged = None
        for inside in range(group):
            head = first + inside
            if diagonal:
                weights = jnp.where(cols_i < rows_i, jnp.exp(scores[inside] + sums[inside]), 0.0)
                carry[:, head : head + 1] = sums[inside][:, 0:1]
            else:
                before = carry[:, head : head + 1]
                weights = jnp.exp(scores[inside] + (sums[inside] + before))
                carry[:, head : head + 1] = before + sums[inside][:, 0:1]
            product = jnp.dot(
                weights.astype(jnp.bfloat16), pair_v, preferred_element_type=jnp.float32
            )
            merged = product if merged is None else jnp.where(lane_owner == inside, product, merged)
        if diagonal:
            acc[:, lanes : lanes + span] = merged
        else:
            acc[:, lanes : lanes + span] += merged


def fused_kernel(
    chips,
    head_count,
    head_width,
    mixer_hbm,
    mixer_gain,
    query_hbm,
    key_hbm,
    value_hbm,
    shift_hbm,
    out_hbm,
    expert_hbm,
    expert_gain,
    routes_ref,
    share_ref,
    gate_hbm,
    up_hbm,
    down_hbm,
    mixer_out,
    expert_out,
    mix_in,
    exp_in,
    normed,
    wq,
    wk,
    wv,
    shift,
    wo,
    wg,
    wu,
    wd,
    rows,
    hidden,
    part,
    part_in,
    pair_out,
    pair_keep,
    pair_in,
    done_out,
    done_keep,
    done_in,
    queries,
    kv,
    heads,
    acc,
    carry,
    upper,
    load_sem,
    far_sem,
    side_sem,
    mate_sem,
    unit_sem,
    part_sem,
    pair_sem,
    done_sem,
    kv_sem,
    head_sem,
    down_sem,
):
    ep, tp = lax.axis_index("ep"), lax.axis_index("tp")
    z, c = ep // 2, ep % 2
    y, x = tp // 2, tp % 2
    tokens, width = exp_in.shape
    length = mix_in.shape[0]
    units = wg.shape[1]
    half = tokens // 2
    cols = head_count * head_width
    mate = {"ep": 2 * z + 1 - c}
    beside = {"tp": 2 * y + 1 - x}
    across = {"tp": 2 * (1 - y) + x}

    def chip_core(chip):
        return {"ep": 2 * chip + c}

    def send(source, target, sems, number, device):
        return pltpu.make_async_remote_copy(
            src_ref=source,
            dst_ref=target,
            send_sem=sems.at[0, number],
            recv_sem=sems.at[1, number],
            device_id=device,
            device_id_type=pl.DeviceIdType.MESH,
        )

    def load(number, source, target):
        return pltpu.make_async_copy(source, target, load_sem.at[number])

    loads = [
        load(0, expert_hbm, exp_in),
        load(1, mixer_hbm, mix_in),
        load(2, query_hbm, wq),
        load(3, key_hbm, wk),
        load(4, value_hbm, wv),
        load(5, shift_hbm, shift),
        load(6, gate_hbm.at[0], wg),
        load(7, up_hbm.at[0], wu),
        load(8, down_hbm.at[0, pl.ds(units * x, units), :], wd.at[x, 0]),
        load(9, down_hbm.at[0, pl.ds(units * (2 + x), units), :], wd.at[x, 1]),
        load(10, out_hbm, wo),
    ]
    for copy in loads[:8]:
        copy.start()

    barrier = pltpu.get_barrier_semaphore()
    pl.semaphore_signal(barrier, inc=1, device_id=mate, device_id_type=pl.DeviceIdType.MESH)
    for step in range(1, 4):
        pl.semaphore_signal(
            barrier, inc=1, device_id={"tp": (tp + step) % 4}, device_id_type=pl.DeviceIdType.MESH
        )
    for step in range(1, chips):
        pl.semaphore_signal(
            barrier,
            inc=1,
            device_id=chip_core((z + step) % chips),
            device_id_type=pl.DeviceIdType.MESH,
        )

    mine = pl.ds(pl.multiple_of(c * tokens, tokens), tokens)
    lanes_i = lax.broadcasted_iota(jnp.int32, (128, 128), 0)
    table = jnp.zeros((128, tokens), jnp.float32)
    for slot in range(routes_ref.shape[0]):
        table = table + jnp.where(
            lanes_i % (2 * chips) == routes_ref[slot : slot + 1, :], share_ref[slot : slot + 1, :], 0.0
        )
    high = table.astype(jnp.bfloat16).astype(jnp.float32)
    table = jnp.where(lanes_i < 2 * chips, high, jnp.where(lanes_i < 4 * chips, table - high, 0.0))
    loads[0].wait()
    step_rows = 32

    def norm_tokens(index, nothing):
        at = pl.multiple_of(index * step_rows, step_rows)
        rows[z, pl.ds(pl.multiple_of(c * tokens + at, step_rows), step_rows), :width] = rms_scale(
            exp_in[pl.ds(at, step_rows), :], expert_gain[...]
        )
        return nothing

    lax.fori_loop(0, tokens // step_rows, norm_tokens, 0, unroll=2)
    rows[z, mine, width:] = table.T.astype(jnp.bfloat16)

    pl.semaphore_wait(barrier, 3 + chips)

    def half_rows(chip, which):
        return rows.at[chip, pl.ds(pl.multiple_of(c * tokens + which * half, half), half), :]

    def mate_half(chip, other):
        which = half_rows(chip, 1 - line if other else line)
        return send(which, which, mate_sem.at[int(other)], chip, mate)

    line = jnp.where(c == 0, y, x)
    facing = {"tp": jnp.where(c == 0, 2 * (1 - y) + x, 2 * y + 1 - x)}

    def far(chip, target, other):
        which = half_rows(chip, 1 - line if other else line)
        return pltpu.make_async_remote_copy(
            src_ref=which,
            dst_ref=which,
            send_sem=far_sem.at[jnp.where(target > z, 1, 0), int(other), chip],
            recv_sem=far_sem.at[2, int(other), chip],
            device_id=chip_core(target % chips),
            device_id_type=pl.DeviceIdType.MESH,
        )

    def side_half(chip):
        return send(half_rows(chip, line), half_rows(chip, line), side_sem, chip, facing)

    up_ok, down_ok = z < chips - 1, z > 0
    for other in (False, True)[: 1 + (HALF_FROM > 1)]:
        pl.when(up_ok)(lambda: far(z, z + 1, other).start())
        pl.when(down_ok)(lambda: far(z, z - 1, other).start())
    mate_half(z, False).start()
    mate_half(z, True).start()

    def down_piece(number):
        return send(
            down_hbm.at[0, pl.ds(units * (2 * number + 1 - x), units), :],
            wd.at[x, number],
            down_sem,
            number,
            beside,
        )

    down_piece(0).start()
    pl.when(c == 0)(lambda: down_piece(1).start())
    for copy in loads[8:]:
        copy.start()

    loads[1].wait()

    def norm_mixer(index, nothing):
        at = pl.ds(pl.multiple_of(index * step_rows, step_rows), step_rows)
        normed[at, :] = rms_scale(mix_in[at, :], mixer_gain[...])
        return nothing

    lax.fori_loop(0, length // step_rows, norm_mixer, 0, unroll=2)

    def kv_far(chip):
        return send(kv.at[2 * chip + c], kv.at[2 * chip + c], kv_sem.at[0], chip, chip_core((z + 1) % chips))

    def kv_mate(chip):
        return send(kv.at[2 * chip + c], kv.at[2 * chip + c], kv_sem.at[1], chip, mate)

    loads[3].wait()
    kv[ep, :, :cols] = jnp.dot(normed[...], wk[...], preferred_element_type=jnp.float32).astype(jnp.bfloat16)
    loads[4].wait()
    kv[ep, :, cols:] = jnp.dot(normed[...], wv[...], preferred_element_type=jnp.float32).astype(jnp.bfloat16)
    pl.when(z == 0)(lambda: kv_far(z).start())
    kv_mate(z).start()
    loads[2].wait()
    queries[...] = jnp.dot(normed[...], wq[...], preferred_element_type=jnp.float32).astype(jnp.bfloat16)
    rows_i = lax.broadcasted_iota(jnp.int32, (2 * length, length), 0)
    cols_i = lax.broadcasted_iota(jnp.int32, (2 * length, length), 1)
    upper[...] = jnp.where(rows_i % length >= cols_i, 1.0, 0.0).astype(jnp.bfloat16)
    loads[5].wait()

    def attend(number, diagonal):
        stick_block(
            head_count, head_width, number, number, diagonal, queries, kv, shift, acc, carry, upper
        )

    near = jnp.minimum(z, chips - 1 - z)

    def chip_at(step):
        index = step - 1
        both = index < 2 * near
        distance = jnp.where(both, index // 2 + 1, index - near + 1)
        below = jnp.where(both, index % 2 == 0, z > chips - 1 - z)
        return jnp.where(step == 0, z, jnp.where(below, z - distance, z + distance))

    def sources(distance):
        return ((z - distance >= 0, z - distance, z + 1), (z + distance < chips, z + distance, z - 1))

    def stage_rows(distance):
        for exists, chip, target in sources(distance):

            @pl.when(exists)
            def _():
                far(chip, z, False).wait_recv()
                mate_half(chip, False).start()

                @pl.when((target >= 0) & (target < chips))
                def _():
                    far(chip, target, False).start()
                    if distance + 1 < HALF_FROM:
                        far(chip, z, True).wait_recv()
                        far(chip, target, True).start()

                if distance >= HALF_FROM:
                    side_half(chip).start()

    def stage_side(distance):
        for exists, chip, target in sources(distance):

            @pl.when(exists)
            def _():
                if distance >= HALF_FROM:
                    side_half(chip).wait_recv()
                elif distance + 1 < HALF_FROM:
                    pl.when((target < 0) | (target >= chips))(lambda: far(chip, z, True).wait_recv())
                else:
                    far(chip, z, True).wait_recv()
                mate_half(chip, True).start()

    def unit_copy(chip):
        return send(hidden.at[chip, y], hidden.at[chip, y], unit_sem, chip, across)

    def stage_units(step):
        chip = chip_at(step)
        mate_half(chip, False).wait_recv()
        mate_half(chip, True).wait_recv()
        lane = lax.broadcasted_iota(jnp.int32, (2 * tokens, 128), 1)
        weight = jnp.sum(
            jnp.where(
                (lane == ep) | (lane == ep + 2 * chips), rows[chip, :, width:].astype(jnp.float32), 0.0
            ),
            axis=1,
            keepdims=True,
        )
        wide = 256
        for first in range(0, units, wide):
            at = slice(first, first + wide)
            gating = jnp.dot(rows[chip, :, :width], wg[:, at], preferred_element_type=jnp.float32)
            linear = jnp.dot(rows[chip, :, :width], wu[:, at], preferred_element_type=jnp.float32)
            gating = jnp.minimum(gating, glu_limit)
            linear = jnp.clip(linear, -glu_limit, glu_limit)
            value = gating * jax.nn.sigmoid(glu_alpha * gating) * (linear + 1.0)
            hidden[chip, y, :, at] = (value * weight).astype(jnp.bfloat16)
        unit_copy(chip).start()

    other_rows = pl.ds(pl.multiple_of((1 - c) * tokens, tokens), tokens)

    def part_copy(chip):
        return send(part.at[chip, :, other_rows, :], part_in.at[chip], part_sem, chip, mate)

    def stage_down(step):
        chip = chip_at(step)
        unit_copy(chip).wait_recv()
        for side in range(2):
            for first in range(0, wd.shape[3], 256):
                at = slice(first, first + 256)
                total = jnp.dot(
                    hidden[chip, 0], wd[side, 0, :, at], preferred_element_type=jnp.float32
                ) + jnp.dot(hidden[chip, 1], wd[side, 1, :, at], preferred_element_type=jnp.float32)
                part[chip, side, :, at] = total.astype(jnp.bfloat16)
        part_copy(chip).start()

    def pair_copy(chip):
        return send(pair_out.at[chip], pair_in.at[chip], pair_sem, chip, beside)

    def stage_pair(step):
        chip = chip_at(step)
        part_copy(chip).wait_recv()
        pair_out[chip] = (
            part[chip, 1 - x, mine, :].astype(jnp.float32) + part_in[chip, 1 - x].astype(jnp.float32)
        ).astype(jnp.bfloat16)
        pair_copy(chip).start()
        pair_keep[chip] = part[chip, x, mine, :].astype(jnp.float32) + part_in[chip, x].astype(jnp.float32)

    def done_copy(chip):
        return pltpu.make_async_remote_copy(
            src_ref=done_out.at[chip],
            dst_ref=done_in.at[z],
            send_sem=done_sem.at[0, chip],
            recv_sem=done_sem.at[1, z],
            device_id=chip_core(chip),
            device_id_type=pl.DeviceIdType.MESH,
        )

    def done_arrived(chip):
        return send(done_out.at[chip], done_in.at[chip], done_sem, chip, chip_core(chip))

    def stage_done(step):
        chip = chip_at(step)
        pair_copy(chip).wait_recv()
        total = pair_keep[chip] + pair_in[chip].astype(jnp.float32)

        @pl.when(chip == z)
        def _():
            done_keep[...] = total

        @pl.when(chip != z)
        def _():
            done_out[chip] = total.astype(jnp.bfloat16)
            done_copy(chip).start()

    def kv_arrive(back):
        chip = z - back
        kv_sent(chip).wait_recv()
        pl.when(up_ok)(lambda: kv_far(chip).start())
        kv_mate(chip).start()

    def kv_sent(chip):
        return send(kv.at[2 * chip + c], kv.at[2 * chip + c], kv_sem.at[0], chip, chip_core((z + 1) % chips))

    def kv_mate_arrived(chip):
        return send(kv.at[2 * chip + 1 - c], kv.at[2 * chip + 1 - c], kv_sem.at[1], chip, mate)

    def attend_chip(back):
        chip = z - back
        kv_mate_arrived(chip).wait_recv()

        @pl.when((back > 0) | (c == 1))
        def _():
            first = jnp.where(back > 0, 1, 0)

            def one(number, nothing):
                attend(2 * chip + first - number, False)
                return nothing

            lax.fori_loop(0, 1 + first, one, 0)

    def head_copy(step):
        other = (tp + step) % 4
        return pltpu.make_async_remote_copy(
            src_ref=heads.at[tp],
            dst_ref=heads.at[tp],
            send_sem=head_sem.at[0, other],
            recv_sem=head_sem.at[1, tp],
            device_id={"tp": other},
            device_id_type=pl.DeviceIdType.MESH,
        )

    def stage_kv_own(distance):
        pl.when((z == distance) & up_ok)(lambda: kv_far(z).start())

    def stage_kv(pair):
        pl.when(z == pair[0])(lambda: kv_arrive(pair[1]))

    def stage_attend(back):
        pl.when(back <= z)(lambda: attend_chip(back))

    def stage_heads(nothing):
        heads[tp] = acc[...].astype(jnp.bfloat16)
        for step in range(1, 4):
            head_copy(step).start()

    def stage_send_down(nothing):
        pl.when(c == 1)(lambda: down_piece(1).start())

    def down_arrived(number):
        return send(wd.at[1 - x, number], wd.at[1 - x, number], down_sem, number, beside)

    def stage_weights(nothing):
        loads[8].wait()
        loads[9].wait()
        down_arrived(0).wait_recv()
        down_arrived(1).wait_recv()

    attend(ep, True)
    loads[6].wait()
    loads[7].wait()
    plan = [(WEIGHTS_AT, stage_weights, 0), (SEND_DOWN_AT, stage_send_down, 0), (HEADS_AT, stage_heads, 0)]
    for chip in range(1, chips):
        for back in range(1, chip + 1):
            plan.append((KV_FROM + KV_HOP * chip + KV_STEP * back, stage_kv, (chip, back)))
    for stage, times in (
        (stage_rows, ROWS_AT),
        (stage_side, SIDE_AT),
        (stage_kv_own, KV_OWN_AT),
        (stage_attend, ATTEND_AT),
        (stage_units, UNITS_AT),
        (stage_down, DOWN_AT),
        (stage_pair, PAIR_AT),
        (stage_done, DONE_AT),
    ):
        for number, time in enumerate(times):
            if time > 0.0 and number < chips:
                plan.append((time, stage, number))
    for _, stage, number in sorted(plan, key=lambda entry: entry[0]):
        stage(number)

    loads[10].wait()
    for step in range(1, 4):
        other = (tp + step) % 4
        send(heads.at[other], heads.at[other], head_sem, other, {"tp": other}).wait_recv()
    for first in range(0, wo.shape[1], 256):
        at = slice(first, first + 256)
        total = jnp.zeros((length, 256), jnp.float32)
        for number in range(4):
            total = total + jnp.dot(
                heads[number], wo[number * cols : (number + 1) * cols, at], preferred_element_type=jnp.float32
            )
        mixer_out[:, at] = total.astype(mixer_out.dtype)
    total = done_keep[...]
    for step in range(1, chips):
        chip = (z + step) % chips
        done_arrived(chip).wait_recv()
        total = total + done_in[chip].astype(jnp.float32)
    expert_out[...] = total.astype(expert_out.dtype)

    down_piece(0).wait_send()
    down_piece(1).wait_send()
    for step in range(1, 4):
        head_copy(step).wait_send()

    def drain(chip, nothing):
        pl.when((chip <= z) & up_ok)(lambda: far(chip, z + 1, False).wait_send())
        pl.when((chip >= z) & down_ok)(lambda: far(chip, z - 1, False).wait_send())
        distance = jnp.abs(chip - z)
        pl.when((chip <= z) & up_ok & (distance + 1 < HALF_FROM))(lambda: far(chip, z + 1, True).wait_send())
        pl.when((chip >= z) & down_ok & (distance + 1 < HALF_FROM))(lambda: far(chip, z - 1, True).wait_send())
        pl.when((chip != z) & (distance >= HALF_FROM))(lambda: side_half(chip).wait_send())
        mate_half(chip, False).wait_send()
        mate_half(chip, True).wait_send()
        unit_copy(chip).wait_send()
        part_copy(chip).wait_send()
        pair_copy(chip).wait_send()
        pl.when(chip != z)(lambda: done_copy(chip).wait_send())
        pl.when((chip <= z) & up_ok)(lambda: kv_far(chip).wait_send())
        pl.when(chip <= z)(lambda: kv_mate(chip).wait_send())
        return nothing

    lax.fori_loop(0, chips, drain, 0)


def fused_layers(
    mixer_rows,
    mixer_gain,
    w_query,
    w_key,
    w_value,
    key_shift,
    w_out,
    expert_rows,
    expert_gain,
    routes,
    route_weight,
    w_gate,
    w_up,
    w_down,
):
    chips = lax.axis_size("ep") // 2
    length, width = mixer_rows.shape
    tokens = expert_rows.shape[0]
    head_count = key_shift.shape[0]
    cols = w_query.shape[1]
    units = w_gate.shape[2]
    outs = w_down.shape[2]
    b16, f32 = jnp.bfloat16, jnp.float32
    vmem = pl.BlockSpec(memory_space=pltpu.VMEM)
    hbm = pl.BlockSpec(memory_space=pl.ANY)
    dma = pltpu.SemaphoreType.DMA
    wide = width + 128
    return pl.pallas_call(
        functools.partial(fused_kernel, chips, head_count, cols // head_count),
        out_shape=(
            jax.ShapeDtypeStruct((length, w_out.shape[1]), b16),
            jax.ShapeDtypeStruct((tokens, outs), b16),
        ),
        in_specs=[hbm, vmem, hbm, hbm, hbm, hbm, hbm, hbm, vmem, vmem, vmem, hbm, hbm, hbm],
        out_specs=(vmem, vmem),
        scratch_shapes=[
            pltpu.VMEM((length, width), b16),
            pltpu.VMEM((tokens, width), b16),
            pltpu.VMEM((length, width), b16),
            pltpu.VMEM(w_query.shape, b16),
            pltpu.VMEM(w_key.shape, b16),
            pltpu.VMEM(w_value.shape, b16),
            pltpu.VMEM(key_shift.shape, f32),
            pltpu.VMEM(w_out.shape, b16),
            pltpu.VMEM(w_gate.shape[1:], b16),
            pltpu.VMEM(w_up.shape[1:], b16),
            pltpu.VMEM((2, 2, units, outs), b16),
            pltpu.VMEM((chips, 2 * tokens, wide), b16),
            pltpu.VMEM((chips, 2, 2 * tokens, units), b16),
            pltpu.VMEM((chips, 2, 2 * tokens, outs), b16),
            pltpu.VMEM((chips, 2, tokens, outs), b16),
            pltpu.VMEM((chips, tokens, outs), b16),
            pltpu.VMEM((chips, tokens, outs), f32),
            pltpu.VMEM((chips, tokens, outs), b16),
            pltpu.VMEM((chips, tokens, outs), b16),
            pltpu.VMEM((tokens, outs), f32),
            pltpu.VMEM((chips, tokens, outs), b16),
            pltpu.VMEM((length, cols), b16),
            pltpu.VMEM((2 * chips, length, 2 * cols), b16),
            pltpu.VMEM((4, length, cols), b16),
            pltpu.VMEM((length, cols), f32),
            pltpu.VMEM((length, max(128, head_count)), f32),
            pltpu.VMEM((2 * length, length), b16),
            dma((11,)),
            dma((3, 2, chips)),
            dma((2, chips)),
            dma((2, 2, chips)),
            dma((2, chips)),
            dma((2, chips)),
            dma((2, chips)),
            dma((2, chips)),
            dma((2, 2, chips)),
            dma((2, 4)),
            dma((2, 2)),
        ],
        compiler_params=pltpu.CompilerParams(
            collective_id=0, has_side_effects=True, vmem_limit_bytes=60 * 1024 * 1024
        ),
    )(
        mixer_rows,
        mixer_gain.reshape(1, -1),
        w_query,
        w_key,
        w_value,
        key_shift,
        w_out,
        expert_rows,
        expert_gain.reshape(1, -1),
        routes.T,
        route_weight.T,
        w_gate,
        w_up,
        w_down,
    )


def earlier_blocks(packed, axis):
    size = lax.axis_size(axis)
    line = [packed]
    for shift in range(2, size, 2):
        line.append(lax.ppermute(packed, axis, [(i, i + shift) for i in range(size - shift)]))
    line = jnp.concatenate(line, axis=0)
    across = lax.ppermute(line, axis, [(i, i ^ 1) for i in range(size)])
    return jnp.concatenate([line, across], axis=0)


def stick_attention(device, queries, gathered, key_shift, head_width):
    length, cols = queries.shape
    head_count = key_shift.shape[0]
    total = gathered.shape[0]
    vmem = pl.BlockSpec(memory_space=pltpu.VMEM)
    return pl.pallas_call(
        functools.partial(stick_kernel, head_count, head_width),
        out_shape=jax.ShapeDtypeStruct((length, cols), jnp.bfloat16),
        in_specs=[pl.BlockSpec(memory_space=pltpu.SMEM), vmem, vmem, vmem],
        out_specs=vmem,
        scratch_shapes=[
            pltpu.VMEM((length, cols), jnp.float32),
            pltpu.VMEM((length, max(128, head_count)), jnp.float32),
            pltpu.VMEM((length, length), jnp.bfloat16),
        ],
        cost_estimate=pl.CostEstimate(
            flops=total * length * head_count * 1500,
            bytes_accessed=gathered.size * 2,
            transcendentals=total * length * head_count * 3,
        ),
    )(device.reshape(1).astype(jnp.int32), queries, gathered, key_shift)


def expert_hidden(flat_rows, gate_cols, upper_cols):
    gating = jnp.minimum(
        jnp.dot(flat_rows, gate_cols, preferred_element_type=jnp.float32), glu_limit
    )
    linear = jnp.clip(
        jnp.dot(flat_rows, upper_cols, preferred_element_type=jnp.float32), -glu_limit, glu_limit
    )
    return (gating * jax.nn.sigmoid(glu_alpha * gating) * (linear + 1.0)).astype(jnp.bfloat16)


def per_device(
    mixer_rows,
    mixer_gain,
    w_query,
    w_key,
    w_value,
    key_shift,
    w_out,
    expert_rows,
    expert_gain,
    routes,
    route_weight,
    w_gate,
    w_up,
    w_down,
):
    length = mixer_rows.shape[0]
    head_count = key_shift.shape[0]
    head_width = w_query.shape[1] // head_count
    if lax.axis_size("tp") == 4 and lax.axis_size("ep") <= 8 and expert_rows.shape[0] == 128:
        return fused_layers(
            mixer_rows,
            mixer_gain,
            w_query,
            w_key,
            w_value,
            key_shift,
            w_out,
            expert_rows,
            expert_gain,
            routes,
            route_weight,
            w_gate,
            w_up,
            w_down,
        )
    normed = rms_scale(mixer_rows, mixer_gain)
    queries = jnp.dot(normed, w_query, preferred_element_type=jnp.float32).astype(jnp.bfloat16)
    key_rows = jnp.dot(normed, w_key, preferred_element_type=jnp.float32).astype(jnp.bfloat16)
    value_rows = jnp.dot(normed, w_value, preferred_element_type=jnp.float32).astype(jnp.bfloat16)
    packed = jnp.concatenate([key_rows, value_rows], axis=1)
    device = lax.axis_index("ep")
    tokens_here, top_count = routes.shape
    expert_count = lax.axis_size("ep")
    capacity = 2 * tokens_here * top_count // expert_count
    rows_after_norm = rms_scale(expert_rows, expert_gain)
    dense = capacity >= tokens_here
    if dense:
        flat_rows = lax.all_gather(rows_after_norm, "ep", axis=0, tiled=True)
        flat_rows, packed, queries = lax.optimization_barrier((flat_rows, packed, queries))
    gathered = earlier_blocks(packed, "ep")
    head_out = stick_attention(device, queries, gathered, key_shift, head_width)
    if dense:
        hidden = expert_hidden(flat_rows, w_gate[0], w_up[0])
        units = lax.all_gather(hidden, "tp", axis=1, tiled=True)
        units, head_out = lax.optimization_barrier((units, head_out))
    weight_rows = w_out
    mixer_out = jnp.dot(
        lax.all_gather(head_out, "tp", axis=1, tiled=True),
        weight_rows,
        preferred_element_type=jnp.float32,
    ).astype(jnp.bfloat16)
    if dense:
        results = jnp.dot(units, w_down[0], preferred_element_type=jnp.float32).astype(jnp.bfloat16)
        leaving = results.reshape(expert_count, tokens_here, results.shape[1])
        returned = lax.all_to_all(leaving, "ep", split_axis=0, concat_axis=0, tiled=True)
        share = jnp.sum(
            jnp.where(
                routes[:, :, None] == jnp.arange(expert_count, dtype=jnp.int32)[None, None, :],
                route_weight[:, :, None],
                0.0,
            ),
            axis=1,
        )
        expert_out = jnp.zeros((tokens_here, results.shape[1]), jnp.float32)
        for number in range(expert_count):
            expert_out = expert_out + share[:, number : number + 1] * returned[number].astype(jnp.float32)
        return (mixer_out, expert_out.astype(jnp.bfloat16))
    chosen = routes.reshape(-1)
    hit_table = (chosen[:, None] == jnp.arange(expert_count, dtype=jnp.int32)[None, :]).astype(
        jnp.int32
    )
    places = jnp.sum((jnp.cumsum(hit_table, axis=0) - 1) * hit_table, axis=1)
    targets = chosen * capacity + places
    assign_ids = jnp.arange(tokens_here * top_count, dtype=jnp.int32) // top_count
    owners = (
        jnp.full((expert_count * capacity,), tokens_here, jnp.int32).at[targets].set(assign_ids)
    )
    padded = jnp.concatenate(
        [rows_after_norm, jnp.zeros((1, rows_after_norm.shape[1]), jnp.bfloat16)], axis=0
    )
    outgoing = padded[owners].reshape(expert_count, capacity, rows_after_norm.shape[1])
    gate_cols = w_gate[0]
    upper_cols = w_up[0]
    down_rows = w_down[0]
    arrived = lax.all_to_all(outgoing, "ep", split_axis=0, concat_axis=0, tiled=True)
    expert_senders, slots_here, feature_count = arrived.shape
    flat_rows = arrived.reshape(expert_senders * slots_here, feature_count)
    gating = jnp.minimum(
        jnp.dot(flat_rows, gate_cols, preferred_element_type=jnp.float32), glu_limit
    )
    linear = jnp.clip(
        jnp.dot(flat_rows, upper_cols, preferred_element_type=jnp.float32), -glu_limit, glu_limit
    )
    hidden = gating * jax.nn.sigmoid(glu_alpha * gating) * (linear + 1.0)
    hidden = hidden.astype(jnp.bfloat16).reshape(expert_senders, slots_here, gate_cols.shape[1])
    senders = hidden.shape[0]
    slot_total = hidden.shape[1]
    portion_units = lax.all_gather(hidden, "tp", axis=2, tiled=True)
    weight_rows = down_rows
    flat_units = portion_units.reshape(senders * slot_total, portion_units.shape[2])
    results = jnp.dot(flat_units, weight_rows, preferred_element_type=jnp.float32)
    leaving = results.astype(jnp.bfloat16).reshape(senders, slot_total, down_rows.shape[1])
    returned = lax.all_to_all(leaving, "ep", split_axis=0, concat_axis=0, tiled=True)
    picked = returned.reshape(expert_count * capacity, down_rows.shape[1])[targets].astype(
        jnp.float32
    )
    picked = picked * route_weight.reshape(-1)[:, None]
    expert_out = jnp.sum(picked.reshape(tokens_here, top_count, down_rows.shape[1]), axis=1).astype(
        jnp.bfloat16
    )
    return (mixer_out, expert_out)


def solution(mesh):
    placed = (
        P("ep", None),
        P(),
        P(None, "tp"),
        P(None, "tp"),
        P(None, "tp"),
        P("tp", None),
        P(None, "tp"),
        P("ep", None),
        P(),
        P("ep", None),
        P("ep", None),
        P("ep", None, "tp"),
        P("ep", None, "tp"),
        P("ep", None, "tp"),
    )
    return jax.shard_map(
        per_device,
        mesh=mesh,
        in_specs=placed,
        out_specs=(P("ep", "tp"), P("ep", "tp")),
        check_vma=False,
    )
```

```python
import functools

import jax
import jax.numpy as jnp
from jax import lax
from jax.experimental import pallas as pl
from jax.experimental.pallas import tpu as pltpu
from jax.sharding import PartitionSpec as P

norm_eps = 1e-06
glu_limit = 7.0
glu_alpha = 1.702
END_ORDER = {
    "units": (7.7, 18.2, 26.0, 34.6),
    "rows": (0.0, 9.5, 17.0, 25.8),
    "side": (0.0, 17.5, 24.5, 34.5),
    "send_down": (9.6, 17.1),
    "lend": (17.2,),
    "borrowed": (27.5,),
    "kv": (0.0, 29.1, 36.0, 39.0),
    "attend": (11.0, 29.8, 38.2, 38.3),
    "weights": (29.5,),
    "down": (29.6, 29.7, 36.1, 40.0),
    "pair": (33.0, 33.1, 38.0, 41.0),
    "done": (42.0, 39.9, 40.9, 48.0),
    "heads": (38.4,),
    "heads_on": (41.1,),
}
MIDDLE_ORDER = {
    "units": (7.7, 19.0, 21.3, 25.0),
    "rows": (0.0, 9.5, 18.3, 25.8),
    "side": (0.0, 18.5, 24.5, 34.5),
    "send_down": (9.65, 18.4),
    "kv_own": (0.0, 9.6, 18.35, 0.0),
    "kv": (0.0, 22.1, 26.9, 39.0),
    "kv_first": (21.2,),
    "attend": (11.0, 29.8, 38.62, 38.63),
    "weights": (29.5,),
    "down": (29.6, 29.7, 33.0, 36.5),
    "pair": (33.5, 33.6, 36.0, 38.6),
    "done": (42.0, 38.7, 38.8, 40.6),
    "heads": (38.65,),
    "heads_on": (41.5,),
}


def rms_scale(source, scaling):
    floats = source.astype(jnp.float32)
    inverse = lax.rsqrt(jnp.mean(floats * floats, axis=-1, keepdims=True) + norm_eps)
    return (floats * inverse * scaling).astype(jnp.bfloat16)


def stick_kernel(head_count, head_width, where_ref, q_ref, kv_ref, shift_ref, out_ref, acc, carry, upper):
    length = q_ref.shape[0]
    device = where_ref[0]
    group = min(head_count, max(1, 128 // head_width))
    span = group * head_width
    cols = head_count * head_width
    rows_i = lax.broadcasted_iota(jnp.int32, (length, length), 0)
    cols_i = lax.broadcasted_iota(jnp.int32, (length, length), 1)
    upper[...] = jnp.where(rows_i >= cols_i, 1.0, 0.0).astype(jnp.bfloat16)
    lane_owner = lax.broadcasted_iota(jnp.int32, (length, span), 1) // head_width

    def block(number, diagonal):
        base = pl.multiple_of(number * length, length)
        half = kv_ref.shape[0] // length // 2
        own_line = (device - number) % 2 == 0
        sibling = device + 1 - 2 * (device % 2)
        slot = jnp.where(own_line, (device - number) // 2, half + (sibling - number) // 2)
        start = pl.multiple_of(slot * length, length)
        for first in range(0, head_count, group):
            lanes = first * head_width
            pair_q = q_ref[:, lanes : lanes + span]
            pair_k = kv_ref[pl.ds(start, length), lanes : lanes + span]
            pair_v = kv_ref[pl.ds(start, length), cols + lanes : cols + lanes + span]
            merged = None
            for inside in range(group):
                head = first + inside
                mine = lane_owner == inside
                q_here = jnp.where(mine, pair_q, jnp.zeros_like(pair_q)) if group > 1 else pair_q
                scores = lax.dot_general(
                    q_here, pair_k, (((1,), (1,)), ((), ())), preferred_element_type=jnp.float32
                )
                scores = scores * head_width ** (-0.5) + shift_ref[head : head + 1, pl.ds(base, length)]
                stay = jnp.minimum(-scores, 0.0) - jnp.log(1.0 + jnp.exp(-jnp.abs(scores)))
                if diagonal:
                    stay = jnp.where(cols_i < rows_i, stay, 0.0)
                high = stay.astype(jnp.bfloat16)
                low = (stay - high.astype(jnp.float32)).astype(jnp.bfloat16)
                inclusive = jnp.dot(high, upper[...], preferred_element_type=jnp.float32)
                inclusive = inclusive + jnp.dot(low, upper[...], preferred_element_type=jnp.float32)
                if diagonal:
                    weights = jnp.where(cols_i < rows_i, jnp.exp(scores + inclusive), 0.0)
                    carry[:, head : head + 1] = inclusive[:, 0:1]
                else:
                    before = carry[:, head : head + 1]
                    weights = jnp.exp(scores + (inclusive + before))
                    carry[:, head : head + 1] = before + inclusive[:, 0:1]
                product = jnp.dot(
                    weights.astype(jnp.bfloat16), pair_v, preferred_element_type=jnp.float32
                )
                merged = product if merged is None else jnp.where(mine, product, merged)
            if diagonal:
                acc[:, lanes : lanes + span] = merged
            else:
                acc[:, lanes : lanes + span] += merged

    block(device, True)

    def earlier(step, nothing):
        block(device - 1 - step, False)
        return nothing

    lax.fori_loop(0, device, earlier, 0)
    out_ref[...] = acc[...].astype(out_ref.dtype)


def stick_block(head_count, head_width, number, slot, diagonal, q_ref, kv_ref, shift_ref, acc, carry, upper):
    length = q_ref.shape[0]
    group = min(head_count, max(1, 128 // head_width))
    span = group * head_width
    cols = head_count * head_width
    rows_i = lax.broadcasted_iota(jnp.int32, (length, length), 0)
    cols_i = lax.broadcasted_iota(jnp.int32, (length, length), 1)
    lane_owner = lax.broadcasted_iota(jnp.int32, (length, span), 1) // head_width
    base = pl.multiple_of(number * length, length)
    for first in range(0, head_count, group):
        lanes = first * head_width
        pair_q = q_ref[:, lanes : lanes + span]
        pair_k = kv_ref[slot, :, lanes : lanes + span]
        pair_v = kv_ref[slot, :, cols + lanes : cols + lanes + span]
        scores, sums = [], []
        for inside in range(group):
            head = first + inside
            q_here = jnp.where(lane_owner == inside, pair_q, jnp.zeros_like(pair_q)) if group > 1 else pair_q
            raw = lax.dot_general(q_here, pair_k, (((1,), (1,)), ((), ())), preferred_element_type=jnp.float32)
            scores.append(raw * head_width ** (-0.5) + shift_ref[head : head + 1, pl.ds(base, length)])
        for inside in range(group):
            score = scores[inside]
            stay = jnp.minimum(-score, 0.0) - jnp.log(1.0 + jnp.exp(-jnp.abs(score)))
            if diagonal:
                stay = jnp.where(cols_i < rows_i, stay, 0.0)
            high = stay.astype(jnp.bfloat16)
            low = (stay - high.astype(jnp.float32)).astype(jnp.bfloat16)
            sums.append(
                jnp.dot(jnp.concatenate([high, low], axis=1), upper[...], preferred_element_type=jnp.float32)
            )
        merged = None
        for inside in range(group):
            head = first + inside
            if diagonal:
                weights = jnp.where(cols_i < rows_i, jnp.exp(scores[inside] + sums[inside]), 0.0)
                carry[:, head : head + 1] = sums[inside][:, 0:1]
            else:
                before = carry[:, head : head + 1]
                weights = jnp.exp(scores[inside] + (sums[inside] + before))
                carry[:, head : head + 1] = before + sums[inside][:, 0:1]
            product = jnp.dot(
                weights.astype(jnp.bfloat16), pair_v, preferred_element_type=jnp.float32
            )
            merged = product if merged is None else jnp.where(lane_owner == inside, product, merged)
        if diagonal:
            acc[:, lanes : lanes + span] = merged
        else:
            acc[:, lanes : lanes + span] += merged


def fused_kernel(
    chips,
    head_count,
    head_width,
    mixer_hbm,
    mixer_gain,
    query_hbm,
    key_hbm,
    value_hbm,
    shift_hbm,
    out_hbm,
    expert_hbm,
    expert_gain,
    routes_ref,
    share_ref,
    gate_hbm,
    up_hbm,
    down_hbm,
    mixer_out,
    expert_out,
    mix_in,
    exp_in,
    normed,
    wq,
    wk,
    wv,
    shift,
    wo,
    wg,
    wu,
    wd,
    rows,
    hidden,
    part,
    part_in,
    pair_out,
    pair_keep,
    pair_in,
    done_out,
    done_keep,
    done_in,
    queries,
    kv,
    heads,
    far_query,
    far_part,
    acc,
    carry,
    upper,
    load_sem,
    far_sem,
    side_sem,
    mate_sem,
    unit_sem,
    part_sem,
    pair_sem,
    done_sem,
    kv_sem,
    head_sem,
    down_sem,
    last_sem,
):
    ep, tp = lax.axis_index("ep"), lax.axis_index("tp")
    z, c = ep // 2, ep % 2
    y, x = tp // 2, tp % 2
    tokens, width = exp_in.shape
    length = mix_in.shape[0]
    units = wg.shape[1]
    half = tokens // 2
    cols = head_count * head_width
    mate = {"ep": 2 * z + 1 - c}
    beside = {"tp": 2 * y + 1 - x}
    across = {"tp": 2 * (1 - y) + x}

    def chip_core(chip):
        return {"ep": 2 * chip + c}

    def send(source, target, sems, number, device):
        return pltpu.make_async_remote_copy(
            src_ref=source,
            dst_ref=target,
            send_sem=sems.at[0, number],
            recv_sem=sems.at[1, number],
            device_id=device,
            device_id_type=pl.DeviceIdType.MESH,
        )

    def load(number, source, target):
        return pltpu.make_async_copy(source, target, load_sem.at[number])

    loads = [
        load(0, expert_hbm, exp_in),
        load(1, mixer_hbm, mix_in),
        load(2, query_hbm, wq),
        load(3, key_hbm, wk),
        load(4, value_hbm, wv),
        load(5, shift_hbm, shift),
        load(6, gate_hbm.at[0], wg),
        load(7, up_hbm.at[0], wu),
        load(8, down_hbm.at[0, pl.ds(units * x, units), :], wd.at[x, 0]),
        load(9, down_hbm.at[0, pl.ds(units * (2 + x), units), :], wd.at[x, 1]),
        load(10, out_hbm, wo),
    ]
    for copy in loads[:8]:
        copy.start()

    barrier = pltpu.get_barrier_semaphore()
    pl.semaphore_signal(barrier, inc=1, device_id=mate, device_id_type=pl.DeviceIdType.MESH)
    for step in range(1, 4):
        pl.semaphore_signal(
            barrier, inc=1, device_id={"tp": (tp + step) % 4}, device_id_type=pl.DeviceIdType.MESH
        )
    for step in range(1, chips):
        pl.semaphore_signal(
            barrier,
            inc=1,
            device_id=chip_core((z + step) % chips),
            device_id_type=pl.DeviceIdType.MESH,
        )

    mine = pl.ds(pl.multiple_of(c * tokens, tokens), tokens)
    lanes_i = lax.broadcasted_iota(jnp.int32, (128, 128), 0)
    table = jnp.zeros((128, tokens), jnp.float32)
    for slot in range(routes_ref.shape[0]):
        table = table + jnp.where(
            lanes_i % (2 * chips) == routes_ref[slot : slot + 1, :], share_ref[slot : slot + 1, :], 0.0
        )
    high = table.astype(jnp.bfloat16).astype(jnp.float32)
    table = jnp.where(lanes_i < 2 * chips, high, jnp.where(lanes_i < 4 * chips, table - high, 0.0))
    loads[0].wait()
    step_rows = 32

    def norm_tokens(index, nothing):
        at = pl.multiple_of(index * step_rows, step_rows)
        rows[z, pl.ds(pl.multiple_of(c * tokens + at, step_rows), step_rows), :width] = rms_scale(
            exp_in[pl.ds(at, step_rows), :], expert_gain[...]
        )
        return nothing

    lax.fori_loop(0, tokens // step_rows, norm_tokens, 0, unroll=2)
    rows[z, mine, width:] = table.T.astype(jnp.bfloat16)

    pl.semaphore_wait(barrier, 3 + chips)

    def half_rows(chip, which):
        return rows.at[chip, pl.ds(pl.multiple_of(c * tokens + which * half, half), half), :]

    def mate_half(chip, other):
        which = half_rows(chip, 1 - line if other else line)
        return send(which, which, mate_sem.at[int(other)], chip, mate)

    line = jnp.where(c == 0, y, x)
    facing = {"tp": jnp.where(c == 0, 2 * (1 - y) + x, 2 * y + 1 - x)}

    def far(chip, target, other):
        which = half_rows(chip, 1 - line if other else line)
        return pltpu.make_async_remote_copy(
            src_ref=which,
            dst_ref=which,
            send_sem=far_sem.at[jnp.where(target > z, 1, 0), int(other), chip],
            recv_sem=far_sem.at[2, int(other), chip],
            device_id=chip_core(target % chips),
            device_id_type=pl.DeviceIdType.MESH,
        )

    def side_half(chip):
        return send(half_rows(chip, line), half_rows(chip, line), side_sem, chip, facing)

    up_ok, down_ok = z < chips - 1, z > 0
    pl.when(up_ok)(lambda: far(z, z + 1, False).start())
    pl.when(down_ok)(lambda: far(z, z - 1, False).start())
    if chips > 2:
        pl.when(z == 0)(lambda: far(z, z + 1, True).start())
        pl.when(z == chips - 1)(lambda: far(z, z - 1, True).start())
    mate_half(z, False).start()
    mate_half(z, True).start()

    def down_piece(number):
        return send(
            down_hbm.at[0, pl.ds(units * (2 * number + 1 - x), units), :],
            wd.at[x, number],
            down_sem,
            number,
            beside,
        )

    @pl.when(c == 0)
    def _():
        down_piece(0).start()
        down_piece(1).start()

    for copy in loads[8:]:
        copy.start()

    loads[1].wait()

    def norm_mixer(index, nothing):
        at = pl.ds(pl.multiple_of(index * step_rows, step_rows), step_rows)
        normed[at, :] = rms_scale(mix_in[at, :], mixer_gain[...])
        return nothing

    lax.fori_loop(0, length // step_rows, norm_mixer, 0, unroll=2)

    def kv_far(chip):
        return send(kv.at[2 * chip + c], kv.at[2 * chip + c], kv_sem.at[0], chip, chip_core((z + 1) % chips))

    def kv_mate(chip):
        return send(kv.at[2 * chip + c], kv.at[2 * chip + c], kv_sem.at[1], chip, mate)

    loads[3].wait()
    kv[ep, :, :cols] = jnp.dot(normed[...], wk[...], preferred_element_type=jnp.float32).astype(jnp.bfloat16)
    loads[4].wait()
    kv[ep, :, cols:] = jnp.dot(normed[...], wv[...], preferred_element_type=jnp.float32).astype(jnp.bfloat16)
    pl.when(z == 0)(lambda: kv_far(z).start())
    kv_mate(z).start()
    loads[2].wait()
    queries[...] = jnp.dot(normed[...], wq[...], preferred_element_type=jnp.float32).astype(jnp.bfloat16)
    rows_i = lax.broadcasted_iota(jnp.int32, (2 * length, length), 0)
    cols_i = lax.broadcasted_iota(jnp.int32, (2 * length, length), 1)
    upper[...] = jnp.where(rows_i % length >= cols_i, 1.0, 0.0).astype(jnp.bfloat16)
    loads[5].wait()

    def attend(number, diagonal):
        stick_block(
            head_count, head_width, number, number, diagonal, queries, kv, shift, acc, carry, upper
        )

    near = jnp.minimum(z, chips - 1 - z)

    def chip_at(step):
        index = step - 1
        both = index < 2 * near
        distance = jnp.where(both, index // 2 + 1, index - near + 1)
        below = jnp.where(both, index % 2 == 0, z > chips - 1 - z)
        return jnp.where(step == 0, z, jnp.where(below, z - distance, z + distance))

    def sources(distance):
        return ((z - distance >= 0, z - distance, z + 1), (z + distance < chips, z + distance, z - 1))

    def whole(chip, distance):
        return ((chip == 0) | (chip == chips - 1)) & (distance == 1) & (chips > 2)

    def stage_rows(distance):
        for exists, chip, target in sources(distance):

            @pl.when(exists)
            def _():
                far(chip, z, False).wait_recv()
                mate_half(chip, False).start()
                pl.when((target >= 0) & (target < chips))(lambda: far(chip, target, False).start())
                pl.when(jnp.logical_not(whole(chip, distance)))(lambda: side_half(chip).start())

    def stage_side(distance):
        for exists, chip, target in sources(distance):

            @pl.when(exists)
            def _():
                pl.when(whole(chip, distance))(lambda: far(chip, z, True).wait_recv())
                pl.when(jnp.logical_not(whole(chip, distance)))(lambda: side_half(chip).wait_recv())
                mate_half(chip, True).start()

    def unit_copy(chip):
        return send(hidden.at[chip, y], hidden.at[chip, y], unit_sem, chip, across)

    def stage_units(step):
        chip = chip_at(step)
        mate_half(chip, False).wait_recv()
        mate_half(chip, True).wait_recv()
        lane = lax.broadcasted_iota(jnp.int32, (2 * tokens, 128), 1)
        weight = jnp.sum(
            jnp.where(
                (lane == ep) | (lane == ep + 2 * chips), rows[chip, :, width:].astype(jnp.float32), 0.0
            ),
            axis=1,
            keepdims=True,
        )
        wide = 256
        for first in range(0, units, wide):
            at = slice(first, first + wide)
            gating = jnp.dot(rows[chip, :, :width], wg[:, at], preferred_element_type=jnp.float32)
            linear = jnp.dot(rows[chip, :, :width], wu[:, at], preferred_element_type=jnp.float32)
            gating = jnp.minimum(gating, glu_limit)
            linear = jnp.clip(linear, -glu_limit, glu_limit)
            value = gating * jax.nn.sigmoid(glu_alpha * gating) * (linear + 1.0)
            hidden[chip, y, :, at] = (value * weight).astype(jnp.bfloat16)
        unit_copy(chip).start()

    other_rows = pl.ds(pl.multiple_of((1 - c) * tokens, tokens), tokens)

    def part_copy(chip):
        return send(part.at[chip, :, other_rows, :], part_in.at[chip], part_sem, chip, mate)

    def stage_down(step):
        chip = chip_at(step)
        unit_copy(chip).wait_recv()
        for side in range(2):
            for first in range(0, wd.shape[3], 256):
                at = slice(first, first + 256)
                total = jnp.dot(
                    hidden[chip, 0], wd[side, 0, :, at], preferred_element_type=jnp.float32
                ) + jnp.dot(hidden[chip, 1], wd[side, 1, :, at], preferred_element_type=jnp.float32)
                part[chip, side, :, at] = total.astype(jnp.bfloat16)
        part_copy(chip).start()

    def pair_copy(chip):
        return send(pair_out.at[chip], pair_in.at[chip], pair_sem, chip, beside)

    def stage_pair(step):
        chip = chip_at(step)
        part_copy(chip).wait_recv()
        pair_out[chip] = (
            part[chip, 1 - x, mine, :].astype(jnp.float32) + part_in[chip, 1 - x].astype(jnp.float32)
        ).astype(jnp.bfloat16)
        pair_copy(chip).start()
        pair_keep[chip] = part[chip, x, mine, :].astype(jnp.float32) + part_in[chip, x].astype(jnp.float32)

    def done_copy(chip):
        return pltpu.make_async_remote_copy(
            src_ref=done_out.at[chip],
            dst_ref=done_in.at[z],
            send_sem=done_sem.at[0, chip],
            recv_sem=done_sem.at[1, z],
            device_id=chip_core(chip),
            device_id_type=pl.DeviceIdType.MESH,
        )

    def done_arrived(chip):
        return send(done_out.at[chip], done_in.at[chip], done_sem, chip, chip_core(chip))

    def stage_done(step):
        chip = chip_at(step)
        pair_copy(chip).wait_recv()
        total = pair_keep[chip] + pair_in[chip].astype(jnp.float32)

        @pl.when(chip == z)
        def _():
            done_keep[...] = total

        @pl.when(chip != z)
        def _():
            done_out[chip] = total.astype(jnp.bfloat16)
            done_copy(chip).start()

    last = chips - 1
    lent = chips > 2

    def kv_goes_up(chip):
        return up_ok & jnp.logical_not((chip == 0) & (z == last - 1) & lent)

    def kv_reaches(chip):
        return jnp.logical_not((chip == 0) & (z == last) & lent)

    def kv_arrive(back):
        chip = z - back
        kv_sent(chip).wait_recv()
        pl.when(kv_goes_up(chip))(lambda: kv_far(chip).start())
        kv_mate(chip).start()

    def kv_sent(chip):
        return send(kv.at[2 * chip + c], kv.at[2 * chip + c], kv_sem.at[0], chip, chip_core((z + 1) % chips))

    def kv_mate_arrived(chip):
        return send(kv.at[2 * chip + 1 - c], kv.at[2 * chip + 1 - c], kv_sem.at[1], chip, mate)

    def attend_chip(back):
        chip = z - back
        kv_mate_arrived(chip).wait_recv()

        @pl.when((back > 0) | (c == 1))
        def _():
            first = jnp.where(back > 0, 1, 0)

            def one(number, nothing):
                attend(2 * chip + first - number, False)
                return nothing

            lax.fori_loop(0, 1 + first, one, 0)

    beside_tp, across_tp = 2 * y + 1 - x, 2 * (1 - y) + x

    def head_copy(number, owner, device):
        return pltpu.make_async_remote_copy(
            src_ref=heads.at[owner],
            dst_ref=heads.at[owner],
            send_sem=head_sem.at[0, number],
            recv_sem=head_sem.at[1, number],
            device_id=device,
            device_id_type=pl.DeviceIdType.MESH,
        )

    def stage_kv_own(distance):
        pl.when((z == distance) & up_ok)(lambda: kv_far(z).start())

    def stage_kv(back):
        if not (lent and back == last):
            pl.when((back <= z) & jnp.logical_not((z == 1) & lent))(lambda: kv_arrive(back))

    def stage_kv_first(nothing):
        pl.when((z == 1) & lent)(lambda: kv_arrive(1))

    def query_copy():
        return send(queries, far_query, last_sem, 0, chip_core(0))

    def part_back():
        return send(far_part.at[0], far_part.at[1], last_sem, 1, chip_core(last))

    def stage_lend(nothing):
        if lent:
            pl.when(z == last)(lambda: query_copy().start())

    def stage_borrowed(nothing):
        if not lent:
            return

        @pl.when(z == 0)
        def _():
            query_copy().wait_recv()
            heads[tp] = acc[...].astype(jnp.bfloat16)
            queries[...] = far_query[...]
            acc[...] = jnp.zeros_like(acc)
            carry[...] = jnp.zeros_like(carry)

            def one(number, nothing):
                attend(1 - number, False)
                return nothing

            lax.fori_loop(0, 2, one, 0)
            far_part[0] = acc[...].astype(jnp.bfloat16)
            part_back().start()

    def stage_attend(back):
        if lent and back == last:

            @pl.when(z == last)
            def _():
                part_back().wait_recv()
                for head in range(head_count):
                    at = slice(head * head_width, (head + 1) * head_width)
                    acc[:, at] += jnp.exp(carry[:, head : head + 1]) * far_part[1, :, at].astype(jnp.float32)
        else:
            pl.when(back <= z)(lambda: attend_chip(back))

    def stage_heads(nothing):
        @pl.when((z > 0) | (not lent))
        def _():
            heads[tp] = acc[...].astype(jnp.bfloat16)

        head_copy(0, tp, beside).start()
        head_copy(1, tp, across).start()

    def stage_heads_on(nothing):
        head_copy(0, tp, beside).wait_recv()
        head_copy(2, beside_tp, across).start()

    def stage_send_down(number):
        if number < 2:
            pl.when(c == 1)(lambda: down_piece(number).start())

    def down_arrived(number):
        return send(wd.at[1 - x, number], wd.at[1 - x, number], down_sem, number, beside)

    def stage_weights(nothing):
        loads[8].wait()
        loads[9].wait()
        down_arrived(0).wait_recv()
        down_arrived(1).wait_recv()

    attend(ep, True)
    loads[6].wait()
    loads[7].wait()
    stages = {
        "weights": stage_weights,
        "send_down": stage_send_down,
        "lend": stage_lend,
        "borrowed": stage_borrowed,
        "rows": stage_rows,
        "side": stage_side,
        "kv_own": stage_kv_own,
        "kv": stage_kv,
        "kv_first": stage_kv_first,
        "attend": stage_attend,
        "units": stage_units,
        "down": stage_down,
        "pair": stage_pair,
        "done": stage_done,
        "heads": stage_heads,
        "heads_on": stage_heads_on,
    }

    def run_order(order):
        plan = []
        for name, times in order.items():
            plan += [(time, name, number) for number, time in enumerate(times) if number < chips]
        for time, name, number in sorted(plan):
            if time > 0.0:
                stages[name](number)

    at_end = down_ok != up_ok
    pl.when(at_end)(lambda: run_order(END_ORDER))
    if chips > 2:
        pl.when(jnp.logical_not(at_end))(lambda: run_order(MIDDLE_ORDER))

    loads[10].wait()
    head_copy(1, tp, across).wait_recv()
    head_copy(2, beside_tp, across).wait_recv()
    for first in range(0, wo.shape[1], 256):
        at = slice(first, first + 256)
        total = jnp.zeros((length, 256), jnp.float32)
        for number in range(4):
            total = total + jnp.dot(
                heads[number], wo[number * cols : (number + 1) * cols, at], preferred_element_type=jnp.float32
            )
        mixer_out[:, at] = total.astype(mixer_out.dtype)
    total = done_keep[...]
    for step in range(1, chips):
        chip = (z + step) % chips
        done_arrived(chip).wait_recv()
        total = total + done_in[chip].astype(jnp.float32)
    expert_out[...] = total.astype(expert_out.dtype)

    down_piece(0).wait_send()
    down_piece(1).wait_send()
    head_copy(0, tp, beside).wait_send()
    head_copy(1, tp, across).wait_send()
    head_copy(2, beside_tp, across).wait_send()

    if lent:
        pl.when(z == last)(lambda: query_copy().wait_send())
        pl.when(z == 0)(lambda: part_back().wait_send())

    def drain(chip, nothing):
        pl.when((chip <= z) & up_ok)(lambda: far(chip, z + 1, False).wait_send())
        pl.when((chip >= z) & down_ok)(lambda: far(chip, z - 1, False).wait_send())
        pl.when((chip == z) & (z == 0) & (chips > 2))(lambda: far(chip, z + 1, True).wait_send())
        pl.when((chip == z) & (z == chips - 1) & (chips > 2))(lambda: far(chip, z - 1, True).wait_send())
        distance = jnp.abs(chip - z)
        pl.when((chip != z) & jnp.logical_not(whole(chip, distance)))(lambda: side_half(chip).wait_send())
        mate_half(chip, False).wait_send()
        mate_half(chip, True).wait_send()
        unit_copy(chip).wait_send()
        part_copy(chip).wait_send()
        pair_copy(chip).wait_send()
        pl.when(chip != z)(lambda: done_copy(chip).wait_send())
        pl.when((chip <= z) & kv_goes_up(chip))(lambda: kv_far(chip).wait_send())
        pl.when((chip <= z) & kv_reaches(chip))(lambda: kv_mate(chip).wait_send())
        return nothing

    lax.fori_loop(0, chips, drain, 0)


def hand_over(mixer_in, expert_in, mixer_out, expert_out):
    mixer_out[...] = mixer_in[...]
    expert_out[...] = expert_in[...]


def fused_layers(
    mixer_rows,
    mixer_gain,
    w_query,
    w_key,
    w_value,
    key_shift,
    w_out,
    expert_rows,
    expert_gain,
    routes,
    route_weight,
    w_gate,
    w_up,
    w_down,
):
    chips = lax.axis_size("ep") // 2
    length, width = mixer_rows.shape
    tokens = expert_rows.shape[0]
    head_count = key_shift.shape[0]
    cols = w_query.shape[1]
    units = w_gate.shape[2]
    outs = w_down.shape[2]
    b16, f32 = jnp.bfloat16, jnp.float32
    vmem = pl.BlockSpec(memory_space=pltpu.VMEM)
    hbm = pl.BlockSpec(memory_space=pl.ANY)
    dma = pltpu.SemaphoreType.DMA
    wide = width + 128
    results = pl.pallas_call(
        functools.partial(fused_kernel, chips, head_count, cols // head_count),
        out_shape=(
            jax.ShapeDtypeStruct((length, w_out.shape[1]), b16),
            jax.ShapeDtypeStruct((tokens, outs), b16),
        ),
        in_specs=[hbm, vmem, hbm, hbm, hbm, hbm, hbm, hbm, vmem, vmem, vmem, hbm, hbm, hbm],
        out_specs=(vmem, vmem),
        scratch_shapes=[
            pltpu.VMEM((length, width), b16),
            pltpu.VMEM((tokens, width), b16),
            pltpu.VMEM((length, width), b16),
            pltpu.VMEM(w_query.shape, b16),
            pltpu.VMEM(w_key.shape, b16),
            pltpu.VMEM(w_value.shape, b16),
            pltpu.VMEM(key_shift.shape, f32),
            pltpu.VMEM(w_out.shape, b16),
            pltpu.VMEM(w_gate.shape[1:], b16),
            pltpu.VMEM(w_up.shape[1:], b16),
            pltpu.VMEM((2, 2, units, outs), b16),
            pltpu.VMEM((chips, 2 * tokens, wide), b16),
            pltpu.VMEM((chips, 2, 2 * tokens, units), b16),
            pltpu.VMEM((chips, 2, 2 * tokens, outs), b16),
            pltpu.VMEM((chips, 2, tokens, outs), b16),
            pltpu.VMEM((chips, tokens, outs), b16),
            pltpu.VMEM((chips, tokens, outs), f32),
            pltpu.VMEM((chips, tokens, outs), b16),
            pltpu.VMEM((chips, tokens, outs), b16),
            pltpu.VMEM((tokens, outs), f32),
            pltpu.VMEM((chips, tokens, outs), b16),
            pltpu.VMEM((length, cols), b16),
            pltpu.VMEM((2 * chips, length, 2 * cols), b16),
            pltpu.VMEM((4, length, cols), b16),
            pltpu.VMEM((length, cols), b16),
            pltpu.VMEM((2, length, cols), b16),
            pltpu.VMEM((length, cols), f32),
            pltpu.VMEM((length, max(128, head_count)), f32),
            pltpu.VMEM((2 * length, length), b16),
            dma((11,)),
            dma((3, 2, chips)),
            dma((2, chips)),
            dma((2, 2, chips)),
            dma((2, chips)),
            dma((2, chips)),
            dma((2, chips)),
            dma((2, chips)),
            dma((2, 2, chips)),
            dma((2, 3)),
            dma((2, 2)),
            dma((2, 2)),
        ],
        compiler_params=pltpu.CompilerParams(
            collective_id=0, has_side_effects=True, vmem_limit_bytes=60 * 1024 * 1024
        ),
    )(
        mixer_rows,
        mixer_gain.reshape(1, -1),
        w_query,
        w_key,
        w_value,
        key_shift,
        w_out,
        expert_rows,
        expert_gain.reshape(1, -1),
        routes.T,
        route_weight.T,
        w_gate,
        w_up,
        w_down,
    )
    return pl.pallas_call(
        hand_over,
        out_shape=tuple(jax.ShapeDtypeStruct(result.shape, b16) for result in results),
        in_specs=[vmem, vmem],
        out_specs=(vmem, vmem),
    )(*results)


def earlier_blocks(packed, axis):
    size = lax.axis_size(axis)
    line = [packed]
    for shift in range(2, size, 2):
        line.append(lax.ppermute(packed, axis, [(i, i + shift) for i in range(size - shift)]))
    line = jnp.concatenate(line, axis=0)
    across = lax.ppermute(line, axis, [(i, i ^ 1) for i in range(size)])
    return jnp.concatenate([line, across], axis=0)


def stick_attention(device, queries, gathered, key_shift, head_width):
    length, cols = queries.shape
    head_count = key_shift.shape[0]
    total = gathered.shape[0]
    vmem = pl.BlockSpec(memory_space=pltpu.VMEM)
    return pl.pallas_call(
        functools.partial(stick_kernel, head_count, head_width),
        out_shape=jax.ShapeDtypeStruct((length, cols), jnp.bfloat16),
        in_specs=[pl.BlockSpec(memory_space=pltpu.SMEM), vmem, vmem, vmem],
        out_specs=vmem,
        scratch_shapes=[
            pltpu.VMEM((length, cols), jnp.float32),
            pltpu.VMEM((length, max(128, head_count)), jnp.float32),
            pltpu.VMEM((length, length), jnp.bfloat16),
        ],
        cost_estimate=pl.CostEstimate(
            flops=total * length * head_count * 1500,
            bytes_accessed=gathered.size * 2,
            transcendentals=total * length * head_count * 3,
        ),
    )(device.reshape(1).astype(jnp.int32), queries, gathered, key_shift)


def expert_hidden(flat_rows, gate_cols, upper_cols):
    gating = jnp.minimum(
        jnp.dot(flat_rows, gate_cols, preferred_element_type=jnp.float32), glu_limit
    )
    linear = jnp.clip(
        jnp.dot(flat_rows, upper_cols, preferred_element_type=jnp.float32), -glu_limit, glu_limit
    )
    return (gating * jax.nn.sigmoid(glu_alpha * gating) * (linear + 1.0)).astype(jnp.bfloat16)


def per_device(
    mixer_rows,
    mixer_gain,
    w_query,
    w_key,
    w_value,
    key_shift,
    w_out,
    expert_rows,
    expert_gain,
    routes,
    route_weight,
    w_gate,
    w_up,
    w_down,
):
    length = mixer_rows.shape[0]
    head_count = key_shift.shape[0]
    head_width = w_query.shape[1] // head_count
    if lax.axis_size("tp") == 4 and lax.axis_size("ep") <= 8 and expert_rows.shape[0] == 128:
        return fused_layers(
            mixer_rows,
            mixer_gain,
            w_query,
            w_key,
            w_value,
            key_shift,
            w_out,
            expert_rows,
            expert_gain,
            routes,
            route_weight,
            w_gate,
            w_up,
            w_down,
        )
    normed = rms_scale(mixer_rows, mixer_gain)
    queries = jnp.dot(normed, w_query, preferred_element_type=jnp.float32).astype(jnp.bfloat16)
    key_rows = jnp.dot(normed, w_key, preferred_element_type=jnp.float32).astype(jnp.bfloat16)
    value_rows = jnp.dot(normed, w_value, preferred_element_type=jnp.float32).astype(jnp.bfloat16)
    packed = jnp.concatenate([key_rows, value_rows], axis=1)
    device = lax.axis_index("ep")
    tokens_here, top_count = routes.shape
    expert_count = lax.axis_size("ep")
    capacity = 2 * tokens_here * top_count // expert_count
    rows_after_norm = rms_scale(expert_rows, expert_gain)
    dense = capacity >= tokens_here
    if dense:
        flat_rows = lax.all_gather(rows_after_norm, "ep", axis=0, tiled=True)
        flat_rows, packed, queries = lax.optimization_barrier((flat_rows, packed, queries))
    gathered = earlier_blocks(packed, "ep")
    head_out = stick_attention(device, queries, gathered, key_shift, head_width)
    if dense:
        hidden = expert_hidden(flat_rows, w_gate[0], w_up[0])
        units = lax.all_gather(hidden, "tp", axis=1, tiled=True)
        units, head_out = lax.optimization_barrier((units, head_out))
    weight_rows = w_out
    mixer_out = jnp.dot(
        lax.all_gather(head_out, "tp", axis=1, tiled=True),
        weight_rows,
        preferred_element_type=jnp.float32,
    ).astype(jnp.bfloat16)
    if dense:
        results = jnp.dot(units, w_down[0], preferred_element_type=jnp.float32).astype(jnp.bfloat16)
        leaving = results.reshape(expert_count, tokens_here, results.shape[1])
        returned = lax.all_to_all(leaving, "ep", split_axis=0, concat_axis=0, tiled=True)
        share = jnp.sum(
            jnp.where(
                routes[:, :, None] == jnp.arange(expert_count, dtype=jnp.int32)[None, None, :],
                route_weight[:, :, None],
                0.0,
            ),
            axis=1,
        )
        expert_out = jnp.zeros((tokens_here, results.shape[1]), jnp.float32)
        for number in range(expert_count):
            expert_out = expert_out + share[:, number : number + 1] * returned[number].astype(jnp.float32)
        return (mixer_out, expert_out.astype(jnp.bfloat16))
    chosen = routes.reshape(-1)
    hit_table = (chosen[:, None] == jnp.arange(expert_count, dtype=jnp.int32)[None, :]).astype(
        jnp.int32
    )
    places = jnp.sum((jnp.cumsum(hit_table, axis=0) - 1) * hit_table, axis=1)
    targets = chosen * capacity + places
    assign_ids = jnp.arange(tokens_here * top_count, dtype=jnp.int32) // top_count
    owners = (
        jnp.full((expert_count * capacity,), tokens_here, jnp.int32).at[targets].set(assign_ids)
    )
    padded = jnp.concatenate(
        [rows_after_norm, jnp.zeros((1, rows_after_norm.shape[1]), jnp.bfloat16)], axis=0
    )
    outgoing = padded[owners].reshape(expert_count, capacity, rows_after_norm.shape[1])
    gate_cols = w_gate[0]
    upper_cols = w_up[0]
    down_rows = w_down[0]
    arrived = lax.all_to_all(outgoing, "ep", split_axis=0, concat_axis=0, tiled=True)
    expert_senders, slots_here, feature_count = arrived.shape
    flat_rows = arrived.reshape(expert_senders * slots_here, feature_count)
    gating = jnp.minimum(
        jnp.dot(flat_rows, gate_cols, preferred_element_type=jnp.float32), glu_limit
    )
    linear = jnp.clip(
        jnp.dot(flat_rows, upper_cols, preferred_element_type=jnp.float32), -glu_limit, glu_limit
    )
    hidden = gating * jax.nn.sigmoid(glu_alpha * gating) * (linear + 1.0)
    hidden = hidden.astype(jnp.bfloat16).reshape(expert_senders, slots_here, gate_cols.shape[1])
    senders = hidden.shape[0]
    slot_total = hidden.shape[1]
    portion_units = lax.all_gather(hidden, "tp", axis=2, tiled=True)
    weight_rows = down_rows
    flat_units = portion_units.reshape(senders * slot_total, portion_units.shape[2])
    results = jnp.dot(flat_units, weight_rows, preferred_element_type=jnp.float32)
    leaving = results.astype(jnp.bfloat16).reshape(senders, slot_total, down_rows.shape[1])
    returned = lax.all_to_all(leaving, "ep", split_axis=0, concat_axis=0, tiled=True)
    picked = returned.reshape(expert_count * capacity, down_rows.shape[1])[targets].astype(
        jnp.float32
    )
    picked = picked * route_weight.reshape(-1)[:, None]
    expert_out = jnp.sum(picked.reshape(tokens_here, top_count, down_rows.shape[1]), axis=1).astype(
        jnp.bfloat16
    )
    return (mixer_out, expert_out)


def solution(mesh):
    placed = (
        P("ep", None),
        P(),
        P(None, "tp"),
        P(None, "tp"),
        P(None, "tp"),
        P("tp", None),
        P(None, "tp"),
        P("ep", None),
        P(),
        P("ep", None),
        P("ep", None),
        P("ep", None, "tp"),
        P("ep", None, "tp"),
        P("ep", None, "tp"),
    )
    return jax.shard_map(
        per_device,
        mesh=mesh,
        in_specs=placed,
        out_specs=(P("ep", "tp"), P("ep", "tp")),
        check_vma=False,
    )
```

```python
import functools

import jax
import jax.numpy as jnp
from jax import lax
from jax.experimental import pallas as pl
from jax.experimental.pallas import tpu as pltpu
from jax.sharding import PartitionSpec as P

norm_eps = 1e-06
glu_limit = 7.0
glu_alpha = 1.702
END_ORDER = {
    "units": (7.7, 18.2, 26.0, 34.6),
    "rows": (0.0, 9.5, 17.0, 25.8),
    "side": (0.0, 17.5, 24.5, 34.5),
    "send_down": (9.6, 17.1),
    "lend": (17.2,),
    "borrowed": (27.5,),
    "kv": (0.0, 29.1, 36.0, 39.0),
    "attend": (11.0, 29.8, 38.2, 38.3),
    "weights": (29.5,),
    "down": (29.6, 29.7, 36.1, 40.0),
    "pair": (33.0, 33.1, 38.0, 41.0),
    "done": (42.0, 39.9, 40.9, 48.0),
    "heads": (38.4,),
    "heads_on": (41.1,),
}
MIDDLE_ORDER = {
    "units": (7.7, 19.0, 21.3, 25.0),
    "rows": (0.0, 9.5, 18.3, 25.8),
    "side": (0.0, 18.5, 24.5, 34.5),
    "send_down": (9.65, 18.4),
    "kv_own": (0.0, 9.6, 18.35, 0.0),
    "kv": (0.0, 22.1, 26.9, 39.0),
    "kv_first": (21.2,),
    "attend": (11.0, 29.8, 38.62, 38.63),
    "weights": (29.5,),
    "down": (29.6, 29.7, 33.0, 36.5),
    "pair": (33.5, 33.6, 36.0, 38.6),
    "done": (42.0, 38.7, 38.8, 40.6),
    "heads": (38.65,),
    "heads_on": (41.5,),
}


def rms_scale(source, scaling):
    floats = source.astype(jnp.float32)
    inverse = lax.rsqrt(jnp.mean(floats * floats, axis=-1, keepdims=True) + norm_eps)
    return (floats * inverse * scaling).astype(jnp.bfloat16)


def stick_kernel(head_count, head_width, where_ref, q_ref, kv_ref, shift_ref, out_ref, acc, carry, upper):
    length = q_ref.shape[0]
    device = where_ref[0]
    group = min(head_count, max(1, 128 // head_width))
    span = group * head_width
    cols = head_count * head_width
    rows_i = lax.broadcasted_iota(jnp.int32, (length, length), 0)
    cols_i = lax.broadcasted_iota(jnp.int32, (length, length), 1)
    upper[...] = jnp.where(rows_i >= cols_i, 1.0, 0.0).astype(jnp.bfloat16)
    lane_owner = lax.broadcasted_iota(jnp.int32, (length, span), 1) // head_width

    def block(number, diagonal):
        base = pl.multiple_of(number * length, length)
        half = kv_ref.shape[0] // length // 2
        own_line = (device - number) % 2 == 0
        sibling = device + 1 - 2 * (device % 2)
        slot = jnp.where(own_line, (device - number) // 2, half + (sibling - number) // 2)
        start = pl.multiple_of(slot * length, length)
        for first in range(0, head_count, group):
            lanes = first * head_width
            pair_q = q_ref[:, lanes : lanes + span]
            pair_k = kv_ref[pl.ds(start, length), lanes : lanes + span]
            pair_v = kv_ref[pl.ds(start, length), cols + lanes : cols + lanes + span]
            merged = None
            for inside in range(group):
                head = first + inside
                mine = lane_owner == inside
                q_here = jnp.where(mine, pair_q, jnp.zeros_like(pair_q)) if group > 1 else pair_q
                scores = lax.dot_general(
                    q_here, pair_k, (((1,), (1,)), ((), ())), preferred_element_type=jnp.float32
                )
                scores = scores * head_width ** (-0.5) + shift_ref[head : head + 1, pl.ds(base, length)]
                stay = jnp.minimum(-scores, 0.0) - jnp.log(1.0 + jnp.exp(-jnp.abs(scores)))
                if diagonal:
                    stay = jnp.where(cols_i < rows_i, stay, 0.0)
                high = stay.astype(jnp.bfloat16)
                low = (stay - high.astype(jnp.float32)).astype(jnp.bfloat16)
                inclusive = jnp.dot(high, upper[...], preferred_element_type=jnp.float32)
                inclusive = inclusive + jnp.dot(low, upper[...], preferred_element_type=jnp.float32)
                if diagonal:
                    weights = jnp.where(cols_i < rows_i, jnp.exp(scores + inclusive), 0.0)
                    carry[:, head : head + 1] = inclusive[:, 0:1]
                else:
                    before = carry[:, head : head + 1]
                    weights = jnp.exp(scores + (inclusive + before))
                    carry[:, head : head + 1] = before + inclusive[:, 0:1]
                product = jnp.dot(
                    weights.astype(jnp.bfloat16), pair_v, preferred_element_type=jnp.float32
                )
                merged = product if merged is None else jnp.where(mine, product, merged)
            if diagonal:
                acc[:, lanes : lanes + span] = merged
            else:
                acc[:, lanes : lanes + span] += merged

    block(device, True)

    def earlier(step, nothing):
        block(device - 1 - step, False)
        return nothing

    lax.fori_loop(0, device, earlier, 0)
    out_ref[...] = acc[...].astype(out_ref.dtype)


def stick_block(head_count, head_width, number, slot, diagonal, q_ref, kv_ref, shift_ref, acc, carry, upper):
    length = q_ref.shape[0]
    group = min(head_count, max(1, 128 // head_width))
    span = group * head_width
    cols = head_count * head_width
    rows_i = lax.broadcasted_iota(jnp.int32, (length, length), 0)
    cols_i = lax.broadcasted_iota(jnp.int32, (length, length), 1)
    lane_owner = lax.broadcasted_iota(jnp.int32, (length, span), 1) // head_width
    base = pl.multiple_of(number * length, length)
    for first in range(0, head_count, group):
        lanes = first * head_width
        pair_q = q_ref[:, lanes : lanes + span]
        pair_k = kv_ref[slot, :, lanes : lanes + span]
        pair_v = kv_ref[slot, :, cols + lanes : cols + lanes + span]
        scores, sums = [], []
        for inside in range(group):
            head = first + inside
            q_here = jnp.where(lane_owner == inside, pair_q, jnp.zeros_like(pair_q)) if group > 1 else pair_q
            raw = lax.dot_general(q_here, pair_k, (((1,), (1,)), ((), ())), preferred_element_type=jnp.float32)
            scores.append(raw * head_width ** (-0.5) + shift_ref[head : head + 1, pl.ds(base, length)])
        for inside in range(group):
            score = scores[inside]
            stay = jnp.minimum(-score, 0.0) - jnp.log(1.0 + jnp.exp(-jnp.abs(score)))
            if diagonal:
                stay = jnp.where(cols_i < rows_i, stay, 0.0)
            high = stay.astype(jnp.bfloat16)
            low = (stay - high.astype(jnp.float32)).astype(jnp.bfloat16)
            sums.append(
                jnp.dot(jnp.concatenate([high, low], axis=1), upper[...], preferred_element_type=jnp.float32)
            )
        merged = None
        for inside in range(group):
            head = first + inside
            if diagonal:
                weights = jnp.where(cols_i < rows_i, jnp.exp(scores[inside] + sums[inside]), 0.0)
                carry[:, head : head + 1] = sums[inside][:, 0:1]
            else:
                before = carry[:, head : head + 1]
                weights = jnp.exp(scores[inside] + (sums[inside] + before))
                carry[:, head : head + 1] = before + sums[inside][:, 0:1]
            product = jnp.dot(
                weights.astype(jnp.bfloat16), pair_v, preferred_element_type=jnp.float32
            )
            merged = product if merged is None else jnp.where(lane_owner == inside, product, merged)
        if diagonal:
            acc[:, lanes : lanes + span] = merged
        else:
            acc[:, lanes : lanes + span] += merged


def fused_kernel(
    chips,
    head_count,
    head_width,
    mixer_hbm,
    mixer_gain,
    query_hbm,
    key_hbm,
    value_hbm,
    shift_hbm,
    out_hbm,
    expert_hbm,
    expert_gain,
    routes_ref,
    share_ref,
    gate_hbm,
    up_hbm,
    down_hbm,
    mixer_out,
    expert_out,
    mix_in,
    exp_in,
    normed,
    wq,
    wk,
    wv,
    shift,
    wo,
    wg,
    wu,
    wd,
    rows,
    hidden,
    part,
    part_in,
    pair_out,
    pair_keep,
    pair_in,
    done_out,
    done_keep,
    done_in,
    queries,
    kv,
    heads,
    far_query,
    far_part,
    acc,
    carry,
    upper,
    load_sem,
    far_sem,
    side_sem,
    mate_sem,
    unit_sem,
    part_sem,
    pair_sem,
    done_sem,
    kv_sem,
    head_sem,
    down_sem,
    last_sem,
):
    ep, tp = lax.axis_index("ep"), lax.axis_index("tp")
    z, c = ep // 2, ep % 2
    y, x = tp // 2, tp % 2
    tokens, width = exp_in.shape
    length = mix_in.shape[0]
    units = wg.shape[1]
    half = tokens // 2
    cols = head_count * head_width
    mate = {"ep": 2 * z + 1 - c}
    beside = {"tp": 2 * y + 1 - x}
    across = {"tp": 2 * (1 - y) + x}

    def chip_core(chip):
        return {"ep": 2 * chip + c}

    def send(source, target, sems, number, device):
        return pltpu.make_async_remote_copy(
            src_ref=source,
            dst_ref=target,
            send_sem=sems.at[0, number],
            recv_sem=sems.at[1, number],
            device_id=device,
            device_id_type=pl.DeviceIdType.MESH,
        )

    def load(number, source, target):
        return pltpu.make_async_copy(source, target, load_sem.at[number])

    loads = [
        load(0, expert_hbm, exp_in),
        load(1, mixer_hbm, mix_in),
        load(2, query_hbm, wq),
        load(3, key_hbm, wk),
        load(4, value_hbm, wv),
        load(5, shift_hbm, shift),
        load(6, gate_hbm.at[0], wg),
        load(7, up_hbm.at[0], wu),
        load(8, down_hbm.at[0, pl.ds(units * x, units), :], wd.at[x, 0]),
        load(9, down_hbm.at[0, pl.ds(units * (2 + x), units), :], wd.at[x, 1]),
        load(10, out_hbm, wo),
    ]
    loads[0].start()

    barrier = pltpu.get_barrier_semaphore()
    pl.semaphore_signal(barrier, inc=1, device_id=mate, device_id_type=pl.DeviceIdType.MESH)
    for step in range(1, 4):
        pl.semaphore_signal(
            barrier, inc=1, device_id={"tp": (tp + step) % 4}, device_id_type=pl.DeviceIdType.MESH
        )
    for step in range(1, chips):
        pl.semaphore_signal(
            barrier,
            inc=1,
            device_id=chip_core((z + step) % chips),
            device_id_type=pl.DeviceIdType.MESH,
        )

    mine = pl.ds(pl.multiple_of(c * tokens, tokens), tokens)
    lanes_i = lax.broadcasted_iota(jnp.int32, (128, 128), 0)
    table = jnp.zeros((128, tokens), jnp.float32)
    for slot in range(routes_ref.shape[0]):
        table = table + jnp.where(
            lanes_i % (2 * chips) == routes_ref[slot : slot + 1, :], share_ref[slot : slot + 1, :], 0.0
        )
    high = table.astype(jnp.bfloat16).astype(jnp.float32)
    table = jnp.where(lanes_i < 2 * chips, high, jnp.where(lanes_i < 4 * chips, table - high, 0.0))
    loads[0].wait()
    for copy in loads[1:8]:
        copy.start()
    step_rows = 32

    def norm_tokens(index, nothing):
        at = pl.multiple_of(index * step_rows, step_rows)
        rows[z, pl.ds(pl.multiple_of(c * tokens + at, step_rows), step_rows), :width] = rms_scale(
            exp_in[pl.ds(at, step_rows), :], expert_gain[...]
        )
        return nothing

    lax.fori_loop(0, tokens // step_rows, norm_tokens, 0, unroll=2)
    rows[z, mine, width:] = table.T.astype(jnp.bfloat16)

    pl.semaphore_wait(barrier, 3 + chips)

    def half_rows(chip, which):
        return rows.at[chip, pl.ds(pl.multiple_of(c * tokens + which * half, half), half), :]

    def mate_half(chip, other):
        which = half_rows(chip, 1 - line if other else line)
        return send(which, which, mate_sem.at[int(other)], chip, mate)

    line = jnp.where(c == 0, y, x)
    facing = {"tp": jnp.where(c == 0, 2 * (1 - y) + x, 2 * y + 1 - x)}

    def far(chip, target, other):
        which = half_rows(chip, 1 - line if other else line)
        return pltpu.make_async_remote_copy(
            src_ref=which,
            dst_ref=which,
            send_sem=far_sem.at[jnp.where(target > z, 1, 0), int(other), chip],
            recv_sem=far_sem.at[2, int(other), chip],
            device_id=chip_core(target % chips),
            device_id_type=pl.DeviceIdType.MESH,
        )

    def side_half(chip):
        return send(half_rows(chip, line), half_rows(chip, line), side_sem, chip, facing)

    up_ok, down_ok = z < chips - 1, z > 0
    pl.when(up_ok)(lambda: far(z, z + 1, False).start())
    pl.when(down_ok)(lambda: far(z, z - 1, False).start())
    if chips > 2:
        pl.when(z == 0)(lambda: far(z, z + 1, True).start())
        pl.when(z == chips - 1)(lambda: far(z, z - 1, True).start())
    mate_half(z, False).start()
    mate_half(z, True).start()

    def down_piece(number):
        return send(
            down_hbm.at[0, pl.ds(units * (2 * number + 1 - x), units), :],
            wd.at[x, number],
            down_sem,
            number,
            beside,
        )

    @pl.when(c == 0)
    def _():
        down_piece(0).start()
        down_piece(1).start()

    for copy in loads[8:]:
        copy.start()

    loads[1].wait()

    def norm_mixer(index, nothing):
        at = pl.ds(pl.multiple_of(index * step_rows, step_rows), step_rows)
        normed[at, :] = rms_scale(mix_in[at, :], mixer_gain[...])
        return nothing

    lax.fori_loop(0, length // step_rows, norm_mixer, 0, unroll=2)

    def kv_far(chip):
        return send(kv.at[2 * chip + c], kv.at[2 * chip + c], kv_sem.at[0], chip, chip_core((z + 1) % chips))

    def kv_mate(chip):
        return send(kv.at[2 * chip + c], kv.at[2 * chip + c], kv_sem.at[1], chip, mate)

    loads[3].wait()
    kv[ep, :, :cols] = jnp.dot(normed[...], wk[...], preferred_element_type=jnp.float32).astype(jnp.bfloat16)
    loads[4].wait()
    kv[ep, :, cols:] = jnp.dot(normed[...], wv[...], preferred_element_type=jnp.float32).astype(jnp.bfloat16)
    pl.when(z == 0)(lambda: kv_far(z).start())
    kv_mate(z).start()
    loads[2].wait()
    queries[...] = jnp.dot(normed[...], wq[...], preferred_element_type=jnp.float32).astype(jnp.bfloat16)
    rows_i = lax.broadcasted_iota(jnp.int32, (2 * length, length), 0)
    cols_i = lax.broadcasted_iota(jnp.int32, (2 * length, length), 1)
    upper[...] = jnp.where(rows_i % length >= cols_i, 1.0, 0.0).astype(jnp.bfloat16)
    loads[5].wait()

    def attend(number, diagonal):
        stick_block(
            head_count, head_width, number, number, diagonal, queries, kv, shift, acc, carry, upper
        )

    near = jnp.minimum(z, chips - 1 - z)

    def chip_at(step):
        index = step - 1
        both = index < 2 * near
        distance = jnp.where(both, index // 2 + 1, index - near + 1)
        below = jnp.where(both, index % 2 == 0, z > chips - 1 - z)
        return jnp.where(step == 0, z, jnp.where(below, z - distance, z + distance))

    def sources(distance):
        return ((z - distance >= 0, z - distance, z + 1), (z + distance < chips, z + distance, z - 1))

    def whole(chip, distance):
        return ((chip == 0) | (chip == chips - 1)) & (distance == 1) & (chips > 2)

    def stage_rows(distance):
        for exists, chip, target in sources(distance):

            @pl.when(exists)
            def _():
                far(chip, z, False).wait_recv()
                mate_half(chip, False).start()
                pl.when((target >= 0) & (target < chips))(lambda: far(chip, target, False).start())
                pl.when(jnp.logical_not(whole(chip, distance)))(lambda: side_half(chip).start())

    def stage_side(distance):
        for exists, chip, target in sources(distance):

            @pl.when(exists)
            def _():
                pl.when(whole(chip, distance))(lambda: far(chip, z, True).wait_recv())
                pl.when(jnp.logical_not(whole(chip, distance)))(lambda: side_half(chip).wait_recv())
                mate_half(chip, True).start()

    def unit_copy(chip):
        return send(hidden.at[chip, y], hidden.at[chip, y], unit_sem, chip, across)

    def stage_units(step):
        chip = chip_at(step)
        mate_half(chip, False).wait_recv()
        mate_half(chip, True).wait_recv()
        lane = lax.broadcasted_iota(jnp.int32, (2 * tokens, 128), 1)
        weight = jnp.sum(
            jnp.where(
                (lane == ep) | (lane == ep + 2 * chips), rows[chip, :, width:].astype(jnp.float32), 0.0
            ),
            axis=1,
            keepdims=True,
        )
        wide = 256
        for first in range(0, units, wide):
            at = slice(first, first + wide)
            gating = jnp.dot(rows[chip, :, :width], wg[:, at], preferred_element_type=jnp.float32)
            linear = jnp.dot(rows[chip, :, :width], wu[:, at], preferred_element_type=jnp.float32)
            gating = jnp.minimum(gating, glu_limit)
            linear = jnp.clip(linear, -glu_limit, glu_limit)
            value = gating * jax.nn.sigmoid(glu_alpha * gating) * (linear + 1.0)
            hidden[chip, y, :, at] = (value * weight).astype(jnp.bfloat16)
        unit_copy(chip).start()

    other_rows = pl.ds(pl.multiple_of((1 - c) * tokens, tokens), tokens)

    def part_copy(chip):
        return send(part.at[chip, :, other_rows, :], part_in.at[chip], part_sem, chip, mate)

    def stage_down(step):
        chip = chip_at(step)
        unit_copy(chip).wait_recv()
        for side in range(2):
            for first in range(0, wd.shape[3], 256):
                at = slice(first, first + 256)
                total = jnp.dot(
                    hidden[chip, 0], wd[side, 0, :, at], preferred_element_type=jnp.float32
                ) + jnp.dot(hidden[chip, 1], wd[side, 1, :, at], preferred_element_type=jnp.float32)
                part[chip, side, :, at] = total.astype(jnp.bfloat16)
        part_copy(chip).start()

    def pair_copy(chip):
        return send(pair_out.at[chip], pair_in.at[chip], pair_sem, chip, beside)

    def stage_pair(step):
        chip = chip_at(step)
        part_copy(chip).wait_recv()
        pair_out[chip] = (
            part[chip, 1 - x, mine, :].astype(jnp.float32) + part_in[chip, 1 - x].astype(jnp.float32)
        ).astype(jnp.bfloat16)
        pair_copy(chip).start()
        pair_keep[chip] = part[chip, x, mine, :].astype(jnp.float32) + part_in[chip, x].astype(jnp.float32)

    def done_copy(chip):
        return pltpu.make_async_remote_copy(
            src_ref=done_out.at[chip],
            dst_ref=done_in.at[z],
            send_sem=done_sem.at[0, chip],
            recv_sem=done_sem.at[1, z],
            device_id=chip_core(chip),
            device_id_type=pl.DeviceIdType.MESH,
        )

    def done_arrived(chip):
        return send(done_out.at[chip], done_in.at[chip], done_sem, chip, chip_core(chip))

    def stage_done(step):
        chip = chip_at(step)
        pair_copy(chip).wait_recv()
        total = pair_keep[chip] + pair_in[chip].astype(jnp.float32)

        @pl.when(chip == z)
        def _():
            done_keep[...] = total

        @pl.when(chip != z)
        def _():
            done_out[chip] = total.astype(jnp.bfloat16)
            done_copy(chip).start()

    last = chips - 1
    lent = chips > 2

    def kv_goes_up(chip):
        return up_ok & jnp.logical_not((chip == 0) & (z == last - 1) & lent)

    def kv_reaches(chip):
        return jnp.logical_not((chip == 0) & (z == last) & lent)

    def kv_arrive(back):
        chip = z - back
        kv_sent(chip).wait_recv()
        pl.when(kv_goes_up(chip))(lambda: kv_far(chip).start())
        kv_mate(chip).start()

    def kv_sent(chip):
        return send(kv.at[2 * chip + c], kv.at[2 * chip + c], kv_sem.at[0], chip, chip_core((z + 1) % chips))

    def kv_mate_arrived(chip):
        return send(kv.at[2 * chip + 1 - c], kv.at[2 * chip + 1 - c], kv_sem.at[1], chip, mate)

    def attend_chip(back):
        chip = z - back
        kv_mate_arrived(chip).wait_recv()

        @pl.when((back > 0) | (c == 1))
        def _():
            first = jnp.where(back > 0, 1, 0)

            def one(number, nothing):
                attend(2 * chip + first - number, False)
                return nothing

            lax.fori_loop(0, 1 + first, one, 0)

    beside_tp, across_tp = 2 * y + 1 - x, 2 * (1 - y) + x

    def head_copy(number, owner, device):
        return pltpu.make_async_remote_copy(
            src_ref=heads.at[owner],
            dst_ref=heads.at[owner],
            send_sem=head_sem.at[0, number],
            recv_sem=head_sem.at[1, number],
            device_id=device,
            device_id_type=pl.DeviceIdType.MESH,
        )

    def stage_kv_own(distance):
        pl.when((z == distance) & up_ok)(lambda: kv_far(z).start())

    def stage_kv(back):
        if not (lent and back == last):
            pl.when((back <= z) & jnp.logical_not((z == 1) & lent))(lambda: kv_arrive(back))

    def stage_kv_first(nothing):
        pl.when((z == 1) & lent)(lambda: kv_arrive(1))

    def query_copy():
        return send(queries, far_query, last_sem, 0, chip_core(0))

    def part_back():
        return send(far_part.at[0], far_part.at[1], last_sem, 1, chip_core(last))

    def stage_lend(nothing):
        if lent:
            pl.when(z == last)(lambda: query_copy().start())

    def stage_borrowed(nothing):
        if not lent:
            return

        @pl.when(z == 0)
        def _():
            query_copy().wait_recv()
            heads[tp] = acc[...].astype(jnp.bfloat16)
            queries[...] = far_query[...]
            acc[...] = jnp.zeros_like(acc)
            carry[...] = jnp.zeros_like(carry)

            def one(number, nothing):
                attend(1 - number, False)
                return nothing

            lax.fori_loop(0, 2, one, 0)
            far_part[0] = acc[...].astype(jnp.bfloat16)
            part_back().start()

    def stage_attend(back):
        if lent and back == last:

            @pl.when(z == last)
            def _():
                part_back().wait_recv()
                for head in range(head_count):
                    at = slice(head * head_width, (head + 1) * head_width)
                    acc[:, at] += jnp.exp(carry[:, head : head + 1]) * far_part[1, :, at].astype(jnp.float32)
        else:
            pl.when(back <= z)(lambda: attend_chip(back))

    def stage_heads(nothing):
        @pl.when((z > 0) | (not lent))
        def _():
            heads[tp] = acc[...].astype(jnp.bfloat16)

        head_copy(0, tp, beside).start()
        head_copy(1, tp, across).start()

    def stage_heads_on(nothing):
        head_copy(0, tp, beside).wait_recv()
        head_copy(2, beside_tp, across).start()

    def stage_send_down(number):
        if number < 2:
            pl.when(c == 1)(lambda: down_piece(number).start())

    def down_arrived(number):
        return send(wd.at[1 - x, number], wd.at[1 - x, number], down_sem, number, beside)

    def stage_weights(nothing):
        loads[8].wait()
        loads[9].wait()
        down_arrived(0).wait_recv()
        down_arrived(1).wait_recv()

    attend(ep, True)
    loads[6].wait()
    loads[7].wait()
    stages = {
        "weights": stage_weights,
        "send_down": stage_send_down,
        "lend": stage_lend,
        "borrowed": stage_borrowed,
        "rows": stage_rows,
        "side": stage_side,
        "kv_own": stage_kv_own,
        "kv": stage_kv,
        "kv_first": stage_kv_first,
        "attend": stage_attend,
        "units": stage_units,
        "down": stage_down,
        "pair": stage_pair,
        "done": stage_done,
        "heads": stage_heads,
        "heads_on": stage_heads_on,
    }

    def run_order(order):
        plan = []
        for name, times in order.items():
            plan += [(time, name, number) for number, time in enumerate(times) if number < chips]
        for time, name, number in sorted(plan):
            if time > 0.0:
                stages[name](number)

    at_end = down_ok != up_ok
    pl.when(at_end)(lambda: run_order(END_ORDER))
    if chips > 2:
        pl.when(jnp.logical_not(at_end))(lambda: run_order(MIDDLE_ORDER))

    loads[10].wait()
    head_copy(1, tp, across).wait_recv()
    head_copy(2, beside_tp, across).wait_recv()
    for first in range(0, wo.shape[1], 256):
        at = slice(first, first + 256)
        total = jnp.zeros((length, 256), jnp.float32)
        for number in range(4):
            total = total + jnp.dot(
                heads[number], wo[number * cols : (number + 1) * cols, at], preferred_element_type=jnp.float32
            )
        mixer_out[:, at] = total.astype(mixer_out.dtype)
    total = done_keep[...]
    for step in range(1, chips):
        chip = (z + step) % chips
        done_arrived(chip).wait_recv()
        total = total + done_in[chip].astype(jnp.float32)
    expert_out[...] = total.astype(expert_out.dtype)

    down_piece(0).wait_send()
    down_piece(1).wait_send()
    head_copy(0, tp, beside).wait_send()
    head_copy(1, tp, across).wait_send()
    head_copy(2, beside_tp, across).wait_send()

    if lent:
        pl.when(z == last)(lambda: query_copy().wait_send())
        pl.when(z == 0)(lambda: part_back().wait_send())

    def drain(chip, nothing):
        pl.when((chip <= z) & up_ok)(lambda: far(chip, z + 1, False).wait_send())
        pl.when((chip >= z) & down_ok)(lambda: far(chip, z - 1, False).wait_send())
        pl.when((chip == z) & (z == 0) & (chips > 2))(lambda: far(chip, z + 1, True).wait_send())
        pl.when((chip == z) & (z == chips - 1) & (chips > 2))(lambda: far(chip, z - 1, True).wait_send())
        distance = jnp.abs(chip - z)
        pl.when((chip != z) & jnp.logical_not(whole(chip, distance)))(lambda: side_half(chip).wait_send())
        mate_half(chip, False).wait_send()
        mate_half(chip, True).wait_send()
        unit_copy(chip).wait_send()
        part_copy(chip).wait_send()
        pair_copy(chip).wait_send()
        pl.when(chip != z)(lambda: done_copy(chip).wait_send())
        pl.when((chip <= z) & kv_goes_up(chip))(lambda: kv_far(chip).wait_send())
        pl.when((chip <= z) & kv_reaches(chip))(lambda: kv_mate(chip).wait_send())
        return nothing

    lax.fori_loop(0, chips, drain, 0)


def hand_over(mixer_in, expert_in, mixer_out, expert_out):
    mixer_out[...] = mixer_in[...]
    expert_out[...] = expert_in[...]


def fused_layers(
    mixer_rows,
    mixer_gain,
    w_query,
    w_key,
    w_value,
    key_shift,
    w_out,
    expert_rows,
    expert_gain,
    routes,
    route_weight,
    w_gate,
    w_up,
    w_down,
):
    chips = lax.axis_size("ep") // 2
    length, width = mixer_rows.shape
    tokens = expert_rows.shape[0]
    head_count = key_shift.shape[0]
    cols = w_query.shape[1]
    units = w_gate.shape[2]
    outs = w_down.shape[2]
    b16, f32 = jnp.bfloat16, jnp.float32
    vmem = pl.BlockSpec(memory_space=pltpu.VMEM)
    hbm = pl.BlockSpec(memory_space=pl.ANY)
    dma = pltpu.SemaphoreType.DMA
    wide = width + 128
    results = pl.pallas_call(
        functools.partial(fused_kernel, chips, head_count, cols // head_count),
        out_shape=(
            jax.ShapeDtypeStruct((length, w_out.shape[1]), b16),
            jax.ShapeDtypeStruct((tokens, outs), b16),
        ),
        in_specs=[hbm, vmem, hbm, hbm, hbm, hbm, hbm, hbm, vmem, vmem, vmem, hbm, hbm, hbm],
        out_specs=(vmem, vmem),
        scratch_shapes=[
            pltpu.VMEM((length, width), b16),
            pltpu.VMEM((tokens, width), b16),
            pltpu.VMEM((length, width), b16),
            pltpu.VMEM(w_query.shape, b16),
            pltpu.VMEM(w_key.shape, b16),
            pltpu.VMEM(w_value.shape, b16),
            pltpu.VMEM(key_shift.shape, f32),
            pltpu.VMEM(w_out.shape, b16),
            pltpu.VMEM(w_gate.shape[1:], b16),
            pltpu.VMEM(w_up.shape[1:], b16),
            pltpu.VMEM((2, 2, units, outs), b16),
            pltpu.VMEM((chips, 2 * tokens, wide), b16),
            pltpu.VMEM((chips, 2, 2 * tokens, units), b16),
            pltpu.VMEM((chips, 2, 2 * tokens, outs), b16),
            pltpu.VMEM((chips, 2, tokens, outs), b16),
            pltpu.VMEM((chips, tokens, outs), b16),
            pltpu.VMEM((chips, tokens, outs), f32),
            pltpu.VMEM((chips, tokens, outs), b16),
            pltpu.VMEM((chips, tokens, outs), b16),
            pltpu.VMEM((tokens, outs), f32),
            pltpu.VMEM((chips, tokens, outs), b16),
            pltpu.VMEM((length, cols), b16),
            pltpu.VMEM((2 * chips, length, 2 * cols), b16),
            pltpu.VMEM((4, length, cols), b16),
            pltpu.VMEM((length, cols), b16),
            pltpu.VMEM((2, length, cols), b16),
            pltpu.VMEM((length, cols), f32),
            pltpu.VMEM((length, max(128, head_count)), f32),
            pltpu.VMEM((2 * length, length), b16),
            dma((11,)),
            dma((3, 2, chips)),
            dma((2, chips)),
            dma((2, 2, chips)),
            dma((2, chips)),
            dma((2, chips)),
            dma((2, chips)),
            dma((2, chips)),
            dma((2, 2, chips)),
            dma((2, 3)),
            dma((2, 2)),
            dma((2, 2)),
        ],
        compiler_params=pltpu.CompilerParams(
            collective_id=0, has_side_effects=True, vmem_limit_bytes=60 * 1024 * 1024
        ),
    )(
        mixer_rows,
        mixer_gain.reshape(1, -1),
        w_query,
        w_key,
        w_value,
        key_shift,
        w_out,
        expert_rows,
        expert_gain.reshape(1, -1),
        routes.T,
        route_weight.T,
        w_gate,
        w_up,
        w_down,
    )
    return pl.pallas_call(
        hand_over,
        out_shape=tuple(jax.ShapeDtypeStruct(result.shape, b16) for result in results),
        in_specs=[vmem, vmem],
        out_specs=(vmem, vmem),
    )(*results)


def earlier_blocks(packed, axis):
    size = lax.axis_size(axis)
    line = [packed]
    for shift in range(2, size, 2):
        line.append(lax.ppermute(packed, axis, [(i, i + shift) for i in range(size - shift)]))
    line = jnp.concatenate(line, axis=0)
    across = lax.ppermute(line, axis, [(i, i ^ 1) for i in range(size)])
    return jnp.concatenate([line, across], axis=0)


def stick_attention(device, queries, gathered, key_shift, head_width):
    length, cols = queries.shape
    head_count = key_shift.shape[0]
    total = gathered.shape[0]
    vmem = pl.BlockSpec(memory_space=pltpu.VMEM)
    return pl.pallas_call(
        functools.partial(stick_kernel, head_count, head_width),
        out_shape=jax.ShapeDtypeStruct((length, cols), jnp.bfloat16),
        in_specs=[pl.BlockSpec(memory_space=pltpu.SMEM), vmem, vmem, vmem],
        out_specs=vmem,
        scratch_shapes=[
            pltpu.VMEM((length, cols), jnp.float32),
            pltpu.VMEM((length, max(128, head_count)), jnp.float32),
            pltpu.VMEM((length, length), jnp.bfloat16),
        ],
        cost_estimate=pl.CostEstimate(
            flops=total * length * head_count * 1500,
            bytes_accessed=gathered.size * 2,
            transcendentals=total * length * head_count * 3,
        ),
    )(device.reshape(1).astype(jnp.int32), queries, gathered, key_shift)


def expert_hidden(flat_rows, gate_cols, upper_cols):
    gating = jnp.minimum(
        jnp.dot(flat_rows, gate_cols, preferred_element_type=jnp.float32), glu_limit
    )
    linear = jnp.clip(
        jnp.dot(flat_rows, upper_cols, preferred_element_type=jnp.float32), -glu_limit, glu_limit
    )
    return (gating * jax.nn.sigmoid(glu_alpha * gating) * (linear + 1.0)).astype(jnp.bfloat16)


def per_device(
    mixer_rows,
    mixer_gain,
    w_query,
    w_key,
    w_value,
    key_shift,
    w_out,
    expert_rows,
    expert_gain,
    routes,
    route_weight,
    w_gate,
    w_up,
    w_down,
):
    length = mixer_rows.shape[0]
    head_count = key_shift.shape[0]
    head_width = w_query.shape[1] // head_count
    if lax.axis_size("tp") == 4 and lax.axis_size("ep") <= 8 and expert_rows.shape[0] == 128:
        return fused_layers(
            mixer_rows,
            mixer_gain,
            w_query,
            w_key,
            w_value,
            key_shift,
            w_out,
            expert_rows,
            expert_gain,
            routes,
            route_weight,
            w_gate,
            w_up,
            w_down,
        )
    normed = rms_scale(mixer_rows, mixer_gain)
    queries = jnp.dot(normed, w_query, preferred_element_type=jnp.float32).astype(jnp.bfloat16)
    key_rows = jnp.dot(normed, w_key, preferred_element_type=jnp.float32).astype(jnp.bfloat16)
    value_rows = jnp.dot(normed, w_value, preferred_element_type=jnp.float32).astype(jnp.bfloat16)
    packed = jnp.concatenate([key_rows, value_rows], axis=1)
    device = lax.axis_index("ep")
    tokens_here, top_count = routes.shape
    expert_count = lax.axis_size("ep")
    capacity = 2 * tokens_here * top_count // expert_count
    rows_after_norm = rms_scale(expert_rows, expert_gain)
    dense = capacity >= tokens_here
    if dense:
        flat_rows = lax.all_gather(rows_after_norm, "ep", axis=0, tiled=True)
        flat_rows, packed, queries = lax.optimization_barrier((flat_rows, packed, queries))
    gathered = earlier_blocks(packed, "ep")
    head_out = stick_attention(device, queries, gathered, key_shift, head_width)
    if dense:
        hidden = expert_hidden(flat_rows, w_gate[0], w_up[0])
        units = lax.all_gather(hidden, "tp", axis=1, tiled=True)
        units, head_out = lax.optimization_barrier((units, head_out))
    weight_rows = w_out
    mixer_out = jnp.dot(
        lax.all_gather(head_out, "tp", axis=1, tiled=True),
        weight_rows,
        preferred_element_type=jnp.float32,
    ).astype(jnp.bfloat16)
    if dense:
        results = jnp.dot(units, w_down[0], preferred_element_type=jnp.float32).astype(jnp.bfloat16)
        leaving = results.reshape(expert_count, tokens_here, results.shape[1])
        returned = lax.all_to_all(leaving, "ep", split_axis=0, concat_axis=0, tiled=True)
        share = jnp.sum(
            jnp.where(
                routes[:, :, None] == jnp.arange(expert_count, dtype=jnp.int32)[None, None, :],
                route_weight[:, :, None],
                0.0,
            ),
            axis=1,
        )
        expert_out = jnp.zeros((tokens_here, results.shape[1]), jnp.float32)
        for number in range(expert_count):
            expert_out = expert_out + share[:, number : number + 1] * returned[number].astype(jnp.float32)
        return (mixer_out, expert_out.astype(jnp.bfloat16))
    chosen = routes.reshape(-1)
    hit_table = (chosen[:, None] == jnp.arange(expert_count, dtype=jnp.int32)[None, :]).astype(
        jnp.int32
    )
    places = jnp.sum((jnp.cumsum(hit_table, axis=0) - 1) * hit_table, axis=1)
    targets = chosen * capacity + places
    assign_ids = jnp.arange(tokens_here * top_count, dtype=jnp.int32) // top_count
    owners = (
        jnp.full((expert_count * capacity,), tokens_here, jnp.int32).at[targets].set(assign_ids)
    )
    padded = jnp.concatenate(
        [rows_after_norm, jnp.zeros((1, rows_after_norm.shape[1]), jnp.bfloat16)], axis=0
    )
    outgoing = padded[owners].reshape(expert_count, capacity, rows_after_norm.shape[1])
    gate_cols = w_gate[0]
    upper_cols = w_up[0]
    down_rows = w_down[0]
    arrived = lax.all_to_all(outgoing, "ep", split_axis=0, concat_axis=0, tiled=True)
    expert_senders, slots_here, feature_count = arrived.shape
    flat_rows = arrived.reshape(expert_senders * slots_here, feature_count)
    gating = jnp.minimum(
        jnp.dot(flat_rows, gate_cols, preferred_element_type=jnp.float32), glu_limit
    )
    linear = jnp.clip(
        jnp.dot(flat_rows, upper_cols, preferred_element_type=jnp.float32), -glu_limit, glu_limit
    )
    hidden = gating * jax.nn.sigmoid(glu_alpha * gating) * (linear + 1.0)
    hidden = hidden.astype(jnp.bfloat16).reshape(expert_senders, slots_here, gate_cols.shape[1])
    senders = hidden.shape[0]
    slot_total = hidden.shape[1]
    portion_units = lax.all_gather(hidden, "tp", axis=2, tiled=True)
    weight_rows = down_rows
    flat_units = portion_units.reshape(senders * slot_total, portion_units.shape[2])
    results = jnp.dot(flat_units, weight_rows, preferred_element_type=jnp.float32)
    leaving = results.astype(jnp.bfloat16).reshape(senders, slot_total, down_rows.shape[1])
    returned = lax.all_to_all(leaving, "ep", split_axis=0, concat_axis=0, tiled=True)
    picked = returned.reshape(expert_count * capacity, down_rows.shape[1])[targets].astype(
        jnp.float32
    )
    picked = picked * route_weight.reshape(-1)[:, None]
    expert_out = jnp.sum(picked.reshape(tokens_here, top_count, down_rows.shape[1]), axis=1).astype(
        jnp.bfloat16
    )
    return (mixer_out, expert_out)


def solution(mesh):
    placed = (
        P("ep", None),
        P(),
        P(None, "tp"),
        P(None, "tp"),
        P(None, "tp"),
        P("tp", None),
        P(None, "tp"),
        P("ep", None),
        P(),
        P("ep", None),
        P("ep", None),
        P("ep", None, "tp"),
        P("ep", None, "tp"),
        P("ep", None, "tp"),
    )
    return jax.shard_map(
        per_device,
        mesh=mesh,
        in_specs=placed,
        out_specs=(P("ep", "tp"), P("ep", "tp")),
        check_vma=False,
    )
```
